256 devices in a mesh: sp: 32 (over z, x), tp: 8 (over y, core).
Axes of the slice: x: 4, y: 4, z: 8, core: 2. Of those that a mesh axis runs over, the one named last changes fastest.
Arguments:
- resid: bfloat16 [12288, 2048], P(('sp', 'tp')), may hold values from -6 to 6
- queries: bfloat16 [12288, 1024], P('sp', 'tp'), may hold values from -6 to 6
- keys: bfloat16 [12288, 1024], P('sp', 'tp'), may hold values from -6 to 6
- values: bfloat16 [12288, 1024], P('sp', 'tp'), may hold values from -6 to 6
- decay_input_part: bfloat16 [12288, 1024], P('sp', 'tp'), may hold values from -4 to 4
- decay_channel_offset: float32 [1024], P('tp'), may hold values from -16 to -2
- decay_head_extra: float32 [12288, 16], P('sp', 'tp'), may hold values from 0 to 0.7
- correction_rate_input: bfloat16 [12288, 1024], P('sp', 'tp'), may hold values from -6 to 6
- correction_rate_offset: float32 [1024], P('tp'), may hold values from -0.4 to 1
- head_norm_gain: float32 [1024], P('tp'), may hold values from 0.1 to 1.9
- mixer_output_weight: bfloat16 [1024, 2048], replicated, may hold values from -0.1875 to 0.1875
- feedforward_norm_gain: float32 [2048], replicated, may hold values from 0.1 to 1.9
- gate_weight: bfloat16 [2048, 5632], P('sp', 'tp'), may hold values from -0.125 to 0.125
- up_weight: bfloat16 [2048, 5632], P('sp', 'tp'), may hold values from -0.125 to 0.125
- down_weight: bfloat16 [5632, 2048], P('tp', 'sp'), may hold values from -0.078125 to 0.078125
Outputs:
- result: bfloat16 [12288, 2048], P(('sp', 'tp'))
The draws below stay inside these ranges and needn't reach their ends.
All inputs are finite; a program needn't handle non-finite values.
Results may differ from the reference program's by a relative error of at most 0.014.
Values may be sent and summed in bfloat16 or wider, within the bound.
A program may use at most 64 MiB of HBM per device.

```python
import math
import jax
import jax.numpy as jnp
from jax import lax

D = 2048
HEADS = 16
HEAD = 64
FF = 5632
TOK_DEV = 384
HW = 1024
TOKENS = 12288
N_SP = 32
N_TP = 8


def head_kinds(key, share):
    chosen = jax.random.uniform(jax.random.fold_in(key, 11), (HEADS,))
    return jnp.repeat(chosen < share, HEAD)


def draw_keys(key, part):
    flips = jax.random.bernoulli(jax.random.fold_in(key, 21), 0.5, (HEADS, HEAD))
    sizes = jax.random.uniform(jax.random.fold_in(key, 22), (HEADS, HEAD), jnp.float32, 0.5, 1.5)
    direction = jnp.where(flips, 1.0, -1.0) * sizes
    turns = jax.random.bernoulli(jax.random.fold_in(key, 23), 0.5, (TOKENS, HEADS))
    amounts = jax.random.uniform(jax.random.fold_in(key, 24), (TOKENS, HEADS), jnp.float32, 1.5, 3.0)
    amplitude = jnp.where(turns, 1.0, -1.0) * amounts
    spread = math.sqrt(6.0 * HEAD / TOKENS)
    noise = spread * jax.random.normal(jax.random.fold_in(key, 25), (TOKENS, HEADS, HEAD), jnp.float32)
    rows = amplitude[:, :, None] * direction[None] + noise
    return jnp.clip(rows, -6.0, 6.0).reshape(TOKENS, HEADS * HEAD).astype(jnp.bfloat16)


def draw_decay_channel_offset(key, part):
    share = 0.5
    slow = head_kinds(key, share)
    jitter = jax.random.uniform(jax.random.fold_in(key, 12), (HEADS * HEAD,), jnp.float32, -0.4, 0.4)
    quick = jax.random.uniform(jax.random.fold_in(key, 18), (HEADS * HEAD,), jnp.float32, -5.6, -2.4)
    return jnp.where(slow, math.log(0.3 / TOKENS) + 0.5 + jitter, quick)


def draw_correction_rate_offset(key, part):
    share = 0.5
    slow = head_kinds(key, share)
    jitter = jax.random.uniform(jax.random.fold_in(key, 13), (HEADS * HEAD,), jnp.float32, -0.4, 0.4)
    strong = jax.random.uniform(jax.random.fold_in(key, 19), (HEADS * HEAD,), jnp.float32, 0.2, 1.0)
    return jnp.where(slow, strong, jitter)


def draw_decay_head_extra(key, part):
    places = jax.random.randint(jax.random.fold_in(key, 14), (3, HEADS), 0, TOKENS)
    losses = jax.random.uniform(jax.random.fold_in(key, 15), (3, HEADS), jnp.float32, 0.22, 0.69)
    positions = jnp.arange(TOKENS, dtype=jnp.int32)[:, None, None]
    return jnp.sum(jnp.where(positions == places[None], losses[None], 0.0), axis=1)


def draw_decay_input_part(key, part):
    noise = 0.5 * jax.random.normal(jax.random.fold_in(key, 16), (TOKENS, HEADS * HEAD), jnp.float32)
    offset = jax.random.uniform(jax.random.fold_in(key, 17), (TOKENS // TOK_DEV, HEADS * HEAD), jnp.float32, -0.7, 0.7)
    return jnp.clip(noise + jnp.repeat(offset, TOK_DEV, axis=0), -4.0, 4.0).astype(jnp.bfloat16)


def steps_of(own_key, shape, split, low, top_value):
    factor_of = 1.0
    for dim, parts in split:
        draws = jax.random.uniform(jax.random.fold_in(jax.random.fold_in(own_key, 6), dim), (parts,), jnp.float32, low / len(split), top_value / len(split))
        factor_of = factor_of * jnp.repeat(jnp.exp(draws), shape[dim] // parts).reshape((-1,) + (1,) * (len(shape) - 1 - dim))
    return factor_of


def gaussian(rng, dims, deviation, reach, pieces=(), held_as=jnp.bfloat16):
    factor_of = steps_of(rng, dims, pieces, -0.22, 0.18) if pieces else 1.0
    array = jax.random.normal(rng, dims, jnp.float32) * deviation * factor_of
    return jnp.minimum(jnp.maximum(array, -reach), reach).astype(held_as)


def setup_inputs(seed: int = 0) -> dict:
    key_of = jax.random.split(jax.random.key(seed), 16)
    resid = gaussian(key_of[0], (TOKENS, D), 1.0, 6.0, ((0, 256),))
    queries = gaussian(key_of[1], (TOKENS, HW), 1.0, 6.0, ((0, 32), (1, 8)))
    keys = draw_keys(jax.random.fold_in(key_of[15], 71), 0)
    values = gaussian(key_of[3], (TOKENS, HW), 1.0, 6.0, ((0, 32), (1, 8)))
    decay_input_part = draw_decay_input_part(jax.random.fold_in(key_of[15], 71), 0)
    decay_channel_offset = draw_decay_channel_offset(jax.random.fold_in(key_of[15], 71), 0)
    decay_head_extra = draw_decay_head_extra(jax.random.fold_in(key_of[15], 71), 0)
    correction_rate_input = gaussian(key_of[7], (TOKENS, HW), 1.0, 6.0, ((0, 32), (1, 8)))
    correction_rate_offset = draw_correction_rate_offset(jax.random.fold_in(key_of[15], 71), 0)
    head_norm_gain = jnp.clip(1.0 + 0.18 * jax.random.normal(key_of[9], (HW,), jnp.float32), 0.1, 1.9)
    mixer_output_weight = gaussian(key_of[10], (HW, D), HW ** -0.5, 0.1875)
    feedforward_norm_gain = jnp.clip(1.0 + 0.18 * jax.random.normal(key_of[11], (D,), jnp.float32), 0.1, 1.9)
    gate_weight = gaussian(key_of[12], (D, FF), D ** -0.5, 0.125, ((0, 32), (1, 8)))
    up_weight = gaussian(key_of[13], (D, FF), D ** -0.5, 0.125, ((0, 32), (1, 8)))
    down_weight = gaussian(key_of[14], (FF, D), FF ** -0.5, 0.078125, ((0, 8), (1, 32)))
    return {"resid": resid, "queries": queries, "keys": keys, "values": values, "decay_input_part": decay_input_part, "decay_channel_offset": decay_channel_offset, "decay_head_extra": decay_head_extra, "correction_rate_input": correction_rate_input, "correction_rate_offset": correction_rate_offset, "head_norm_gain": head_norm_gain, "mixer_output_weight": mixer_output_weight, "feedforward_norm_gain": feedforward_norm_gain, "gate_weight": gate_weight, "up_weight": up_weight, "down_weight": down_weight}


def recurrence(carry_state, inputs):
    query_t, decay_t, key_t, value_t, unit_t, lrate_t = inputs
    lifted = jnp.einsum('hvk,hk->hv', carry_state, -unit_t, precision=lax.Precision.HIGHEST)
    carry_state = carry_state * decay_t[:, None, :] + lifted[:, :, None] * (unit_t * lrate_t)[:, None, :] + value_t[:, :, None] * key_t[:, None, :]
    return (carry_state, jnp.einsum('hvk,hk->hv', carry_state, query_t, precision=lax.Precision.HIGHEST))

def reference(resid, queries, keys, values, decay_input_part, decay_channel_offset, decay_head_extra, correction_rate_input, correction_rate_offset, head_norm_gain, mixer_output_weight, feedforward_norm_gain, gate_weight, up_weight, down_weight):

    def head_count(arr):
        return arr.astype(jnp.float32).reshape(TOKENS, HEADS, HEAD)
    correction_rate = jnp.exp(-jax.nn.softplus(-(decay_channel_offset + decay_input_part.astype(jnp.float32))) - 0.5)
    decay_factor = jnp.exp(-head_count(correction_rate) - decay_head_extra[:, :, None])
    key_f = head_count(keys)
    unit_keys = key_f * lax.rsqrt(lax.optimization_barrier(jnp.sum(key_f * key_f, axis=-1, keepdims=True)) + 1e-06)
    lrate = head_count(jax.nn.sigmoid(correction_rate_offset + correction_rate_input.astype(jnp.float32)))
    start = jnp.zeros((HEADS, HEAD, HEAD), jnp.float32)
    _, mixer_out = lax.scan(recurrence, start, (head_count(queries), decay_factor, key_f, head_count(values), unit_keys, lrate))
    center = mixer_out - lax.optimization_barrier(jnp.mean(mixer_out, axis=-1, keepdims=True))
    spread = lax.optimization_barrier(jnp.mean(center * center, axis=-1, keepdims=True))
    mixed = (center * lax.rsqrt(spread + 1e-05) * head_norm_gain.reshape(HEADS, HEAD)).reshape(TOKENS, HW).astype(jnp.bfloat16)

    def layer_block(pair):
        mixed_rows, resid_rows = pair
        proj = jnp.dot(mixed_rows, mixer_output_weight, preferred_element_type=jnp.float32)
        resid_mid = (resid_rows.astype(jnp.float32) + proj).astype(jnp.bfloat16)
        mid_f = resid_mid.astype(jnp.float32)
        normed = (mid_f * lax.rsqrt(lax.optimization_barrier(jnp.mean(mid_f * mid_f, axis=-1, keepdims=True)) + 1e-06) * feedforward_norm_gain).astype(jnp.bfloat16)
        gate = jnp.dot(normed, gate_weight, preferred_element_type=jnp.float32)
        upper = jnp.dot(normed, up_weight, preferred_element_type=jnp.float32)
        hidden = (jax.nn.silu(gate) * upper).astype(jnp.bfloat16)
        hid_parts = hidden.reshape(TOK_DEV, N_TP, FF // N_TP).astype(jnp.float32)
        down_parts = down_weight.reshape(N_TP, FF // N_TP, D).astype(jnp.float32)
        partial_value = jnp.einsum('tnf,nfd->ntd', hid_parts, down_parts).astype(jnp.bfloat16)
        partial_value = lax.optimization_barrier(partial_value).astype(jnp.float32)
        down_sum = lax.optimization_barrier(jnp.sum(partial_value, axis=0))
        return (mid_f + 0.5 * down_sum).astype(jnp.bfloat16)
    result = lax.map(layer_block, (mixed.reshape(N_SP, TOK_DEV, HW), resid.reshape(N_SP, TOK_DEV, D)))
    return result.reshape(TOKENS, D)
```

```python
import functools

import jax
import jax.numpy as jnp
from jax import lax
from jax.experimental import pallas as pl
from jax.experimental.pallas import tpu as pltpu
from jax.sharding import Mesh
from jax.sharding import PartitionSpec as P

F32, BF16 = jnp.float32, jnp.bfloat16
MESH = pl.DeviceIdType.MESH
HEAD, LANES, CH = 64, 128, 64
NZ, NX, NY, NC = 8, 4, 4, 2
NT = NY * NC
CHUNKS = 6
GROUP = 3
COLS = 4
SP, TP, SP_TP = ("z", "x"), ("y", "c"), ("z", "x", "y", "c")


def dg(a, b, ca=1, cb=0):
    return lax.dot_general(a, b, (((ca,), (cb,)), ((), ())), preferred_element_type=F32)


def halves(x):
    hi = x.astype(BF16)
    return hi, (x - hi.astype(F32)).astype(BF16)


def mm(a, b, ca=1, cb=0):
    return dg(a[0], b[0], ca, cb) + dg(a[0], b[1], ca, cb) + dg(a[1], b[0], ca, cb)


def thirds(x):
    hi = x.astype(BF16)
    rest = x - hi.astype(F32)
    mid = rest.astype(BF16)
    return hi, mid, (rest - mid.astype(F32)).astype(BF16)


def iota(shape, dim):
    return lax.broadcasted_iota(jnp.int32, shape, dim)


def first_head(rows):
    return iota((rows, LANES), 1) < HEAD


def stacked(x):
    own = first_head(x.shape[0])
    zero = jnp.zeros_like(x)
    return jnp.concatenate([jnp.where(own, x, zero), jnp.where(own, zero, x)], axis=0)


def folded(x):
    half = x.shape[0] // 2
    return x[:half] + x[half:]


def head_ones():
    return (iota((LANES, LANES), 0) // HEAD == iota((LANES, LANES), 1) // HEAD).astype(BF16)


def head_sum(x, ones):
    hi, lo = halves(x)
    return dg(hi, ones) + dg(lo, ones)


def sigmoid(x):
    return 1.0 / (1.0 + jnp.exp(-x))


def mixer_group(first, q_ref, k_ref, v_ref, dip_ref, cri_ref, dco_ref, cro_ref, extra_ref, m_ref, n_ref, r_ref, o_ref):
    ids = range(first, first + GROUP)
    ones = head_ones()
    row, col = iota((LANES, LANES), 0), iota((LANES, LANES), 1)
    eye = (row == col).astype(F32)
    low = (iota((CH, CH), 0) >= iota((CH, CH), 1)).astype(BF16)
    ends, us, bts, avs, reads, vs = [], [], [], [], [], []
    invs, offs, qks = [], [], []
    for c in ids:
        rows = pl.ds(c * CH, CH)
        q, k, v = (r[rows, :].astype(F32) for r in (q_ref, k_ref, v_ref))
        pre = dco_ref[...] + dip_ref[rows, :].astype(F32)
        log_decay = -(sigmoid(pre) * 0.6065306597126334) - extra_ref[rows, :]
        unit = k * lax.rsqrt(head_sum(k * k, ones) + 1e-6)
        b = unit * sigmoid(cro_ref[...] + cri_ref[rows, :].astype(F32))
        total = sum(dg(low, part) for part in thirds(log_decay))
        before = total - log_decay
        mid, end = total[CH // 2 - 1 : CH // 2], total[CH - 1 :]
        up, down = jnp.exp(total - mid), jnp.exp(mid - total)
        up_before = jnp.exp(before - mid)
        rest = jnp.exp(end - total)
        left = halves(jnp.concatenate([stacked(unit * up_before), stacked(q * up)], axis=0))
        right = halves(jnp.concatenate([stacked(k * down), stacked(b * down)], axis=0))
        a = mm(left, right, 1, 1)
        a_uk = jnp.where(row > col, a[:LANES, :LANES], 0.0)
        a_qk = jnp.where(row >= col, a[LANES:, :LANES], 0.0)
        a_qb = jnp.where(row >= col, a[LANES:, LANES:], 0.0)
        offs.append(a[:LANES, LANES:])
        vst = halves(stacked(v))
        av = mm(halves(jnp.concatenate([a_uk, a_qk], axis=0)), vst)
        us.append(halves(jnp.concatenate([stacked(unit * jnp.exp(before)), av[:LANES]], axis=1)))
        avs.append(av[LANES:])
        qks.append(halves(a_qb))
        reads.append(stacked(q * jnp.exp(total)))
        bts.append(halves(stacked(b * rest)))
        ends.append((jnp.exp(end), mm(vst, halves(stacked(k * rest)), 0, 0)))
    size = 1
    while size < CH:
        inside = (row // (2 * size) == col // (2 * size)) & (row // size != col // size) & (row > col)
        for i in range(GROUP):
            part = jnp.where(inside, offs[i], 0.0)
            if size == 1:
                invs.append(eye - part)
            else:
                inv = halves(invs[i])
                invs[i] = invs[i] - mm(halves(mm(inv, halves(part))), inv)
        size *= 2
    for i, c in enumerate(ids):
        wu = mm(halves(invs[i]), us[i])
        wu2 = halves(wu)
        ro = mm(qks[i], wu2)
        r_ref[c] = reads[i] - ro[:, :LANES]
        o_ref[c] = avs[i] - ro[:, LANES:]
        mn = mm(wu2, bts[i], 0, 0)
        decay, kv = ends[i]
        m_ref[c] = jnp.where(row == col, decay, 0.0) - mn[:LANES]
        n_ref[c] = kv - mn[LANES:]


def unpacked(message):
    wide = message.astype(F32)
    return stacked(wide[:HEAD]).astype(BF16), stacked(wide[HEAD:])


def packed(trans, state):
    return jnp.concatenate([folded(trans), folded(state)], axis=0).astype(BF16)


def after(total, message):
    trans, state = unpacked(message)
    hi, lo = halves(total)
    out = dg(hi, trans) + dg(lo, trans)
    return jnp.concatenate([out[:LANES], out[LANES:] + state], axis=0)


class Gather:
    def __init__(self, bufs, send_z, recv_z, send_x, recv_x, sends):
        self.bufs, self.sends = bufs, sends
        self.send_z, self.recv_z, self.send_x, self.recv_x = send_z, recv_z, send_x, recv_x
        self.z, self.x = lax.axis_index("z"), lax.axis_index("x")

    def at(self, w, dz, dx, part=None):
        ref = self.bufs[w].at[lax.rem(self.z + dz + NZ, NZ), lax.rem(self.x + dx + NX, NX)]
        rows = ref.shape[0] // 2
        return ref if part is None else ref.at[pl.ds(part * rows, rows)]

    def along_z(self, ring, w, dx, hop, right):
        sign = 1 if right else -1
        part = None if hop < 4 else (0 if right else 1)
        ref = self.at(w, -sign * (hop - 1), dx, part)
        slot = hop - 1 + (0 if right else 4)
        return pltpu.make_async_remote_copy(
            ref, ref, self.send_z.at[ring, slot], self.recv_z.at[ring, slot],
            device_id={"z": lax.rem(self.z + sign + NZ, NZ)}, device_id_type=MESH,
        )

    def got_z(self, ring, w, dx, hop, right):
        sign = 1 if right else -1
        part = None if hop < 4 else (0 if right else 1)
        ref = self.at(w, -sign * hop, dx, part)
        slot = hop - 1 + (0 if right else 4)
        pltpu.make_async_remote_copy(
            ref, ref, self.send_z.at[ring, slot], self.recv_z.at[ring, slot],
            device_id={"z": lax.rem(self.z + sign + NZ, NZ)}, device_id_type=MESH,
        ).wait_recv()

    def along_x(self, ring, w, dz, hop, right):
        sign = 1 if right else -1
        part = None if hop < 2 else (0 if right else 1)
        ref = self.at(w, dz, -sign * (hop - 1), part)
        slot = hop - 1 + (0 if right else 2)
        return pltpu.make_async_remote_copy(
            ref, ref, self.send_x.at[ring, slot], self.recv_x.at[ring, slot],
            device_id={"x": lax.rem(self.x + sign + NX, NX)}, device_id_type=MESH,
        )

    def got_x(self, ring, w, dz, hop, right):
        sign = 1 if right else -1
        part = None if hop < 2 else (0 if right else 1)
        ref = self.at(w, dz, -sign * hop, part)
        slot = hop - 1 + (0 if right else 2)
        pltpu.make_async_remote_copy(
            ref, ref, self.send_x.at[ring, slot], self.recv_x.at[ring, slot],
            device_id={"x": lax.rem(self.x + sign + NX, NX)}, device_id_type=MESH,
        ).wait_recv()

    def go(self, copy):
        copy.start()
        self.sends.append(copy)

    def z_hop(self, ring, w, dx, hop):
        for right in (True, False):
            self.go(self.along_z(ring, w, dx, hop, right))

    def x_hop(self, ring, w, dz, hop):
        for right in (True, False):
            self.go(self.along_x(ring, w, dz, hop, right))

    def z_got(self, ring, w, dx, hop):
        for right in (True, False):
            self.got_z(ring, w, dx, hop, right)

    def x_got(self, ring, w, dz, hop):
        for right in (True, False):
            self.got_x(ring, w, dz, hop, right)


DZ = (0, -1, 1, -2, 2, -3, 3, 4)
DX = (0, 1, -1, 2)


def stages(g):
    def start():
        for w, ring in ((1, 0), (2, 1)):
            g.z_hop(ring, w, 0, 1)
        g.x_hop(16, 0, 0, 1)
        g.z_hop(2, 0, 0, 1)
        for w in (1, 2):
            g.x_hop(8 * (w - 1), w, 0, 1)

    def z_round(hop):
        for w, ring in ((1, 0), (2, 1)):
            g.z_got(ring, w, 0, hop)
            if hop < 4:
                g.z_hop(ring, w, 0, hop + 1)
                for i in (2 * hop - 1, 2 * hop):
                    g.x_hop(8 * (w - 1) + i, w, DZ[i], 1)
            else:
                g.x_hop(8 * (w - 1) + 7, w, 4, 1)

    def x_first():
        g.x_got(16, 0, 0, 1)
        g.x_hop(16, 0, 0, 2)
        for i in (1, 2):
            g.z_hop(2 + i, 0, DX[i], 1)

    def x_second():
        g.x_got(16, 0, 0, 2)
        g.z_hop(5, 0, 2, 1)

    def x_forward(i):
        for w in (1, 2):
            g.x_got(8 * (w - 1) + i, w, DZ[i], 1)
            g.x_hop(8 * (w - 1) + i, w, DZ[i], 2)

    def g_round(i, hop):
        g.z_got(2 + i, 0, DX[i], hop)
        if hop < 4:
            g.z_hop(2 + i, 0, DX[i], hop + 1)

    def x_last(i):
        for w in (1, 2):
            g.x_got(8 * (w - 1) + i, w, DZ[i], 2)

    return start, z_round, x_first, x_second, x_forward, g_round, x_last


def kernel(
    q_ref, k_ref, v_ref, dip_ref, cri_ref, dco_ref, cro_ref, gain_ref, extra_ref, fng_ref,
    resid_hbm, wo_hbm, gate_hbm, up_hbm, down_hbm,
    out_ref,
    wg, wu, wd, wo, resid,
    m_ref, n_ref, r_ref, o_ref, gm_ref, hm_ref,
    tot_ref, xbuf, xpre, zsrc, zbuf, s_ref,
    mixed_ref, rowmix, mid_ref, rows, hid_ref,
    own_part, full_part, sib_src, sib_buf, y_src, y_buf,
    local_sem, send_z, recv_z, send_x, recv_x,
    st_send, st_recv, a2a_send, a2a_recv, ag_send, ag_recv, rs_send, rs_recv,
):
    z, x, y, c = (lax.axis_index(n) for n in SP_TP)
    tp = y * NC + c
    sends = []
    own = [
        pltpu.make_async_copy(src, dst, local_sem.at[i])
        for i, (src, dst) in enumerate(
            ((up_hbm, wu.at[z, x]), (down_hbm, wd.at[z, x]), (gate_hbm, wg.at[z, x]), (wo_hbm, wo), (resid_hbm, resid))
        )
    ]
    for copy in own:
        copy.start()

    barrier = pltpu.get_barrier_semaphore()
    peers = [{"x": lax.rem(x + d, NX)} for d in range(1, NX)]
    peers += [{"z": lax.rem(z + d, NZ)} for d in range(1, NZ)]
    peers += [{"y": lax.rem(tp + d, NT) // NC, "c": lax.rem(tp + d, NT) % NC} for d in range(1, NT)]
    for peer in peers:
        pl.semaphore_signal(barrier, inc=1, device_id=peer, device_id_type=MESH)
    pl.semaphore_wait(barrier, len(peers))

    g = Gather((wg, wu, wd), send_z, recv_z, send_x, recv_x, sends)
    start, z_round, x_first, x_second, x_forward, g_round, x_last = stages(g)
    for copy in own[:3]:
        copy.wait()
    start()

    mix = functools.partial(
        mixer_group, q_ref=q_ref, k_ref=k_ref, v_ref=v_ref, dip_ref=dip_ref, cri_ref=cri_ref, dco_ref=dco_ref,
        cro_ref=cro_ref, extra_ref=extra_ref, m_ref=m_ref, n_ref=n_ref, r_ref=r_ref, o_ref=o_ref,
    )
    mix(0)
    x_first()
    z_round(1)
    mix(GROUP)
    x_second()
    z_round(2)

    row, col = iota((LANES, LANES), 0), iota((LANES, LANES), 1)
    total = jnp.concatenate([(row == col).astype(F32), jnp.zeros((LANES, LANES), F32)], axis=0)
    for i in range(CHUNKS):
        split = halves(total)
        gh = mm(halves(r_ref[i]), split, 1, 1)
        rows_i = pl.ds(i * CH, CH)
        gm_ref[rows_i, :] = folded(gh[:, :LANES])
        hm_ref[rows_i, :] = folded(gh[:, LANES:] + o_ref[i])
        step = mm(split, halves(m_ref[i]))
        total = jnp.concatenate([step[:LANES], step[LANES:] + n_ref[i]], axis=0)
    tot_ref[...] = packed(total[:LANES], total[LANES:])
    for d in range(1, NX):
        copy = pltpu.make_async_remote_copy(
            tot_ref, xbuf.at[d - 1], st_send.at[d - 1], st_recv.at[d - 1],
            device_id={"x": lax.rem(x + d, NX)}, device_id_type=MESH,
        )
        copy.start()
        sends.append(copy)
    x_forward(0)
    for d in range(1, NX):
        pltpu.make_async_remote_copy(
            tot_ref, xbuf.at[d - 1], st_send.at[d - 1], st_recv.at[d - 1],
            device_id={"x": lax.rem(x + d, NX)}, device_id_type=MESH,
        ).wait_recv()
    total = jnp.concatenate([(row == col).astype(F32), jnp.zeros((LANES, LANES), F32)], axis=0)
    prefix = total
    for i in range(NX):
        prefix = jnp.where(x == i, total, prefix)
        message = tot_ref[...]
        for d in range(1, NX):
            message = jnp.where(lax.rem(x - i + NX, NX) == d, xbuf[d - 1], message)
        total = after(total, message)
    xpre[...] = prefix
    zsrc[...] = packed(total[:LANES], total[LANES:])

    def z_state(d):
        return pltpu.make_async_remote_copy(
            zsrc, zbuf.at[d - 1], st_send.at[2 + d], st_recv.at[2 + d],
            device_id={"z": lax.rem(z + d, NZ)}, device_id_type=MESH,
        )

    for d in range(1, NZ):
        pl.when(z + d < NZ)(lambda d=d: z_state(d).start())
    z_round(3)
    s_ref[...] = jnp.zeros_like(s_ref)
    for d in range(NZ - 1, 0, -1):

        @pl.when(z >= d)
        def _(d=d):
            z_state(d).wait_recv()
            trans, state = unpacked(zbuf[d - 1])
            hi, lo = halves(s_ref[...])
            s_ref[...] = dg(hi, trans) + dg(lo, trans) + state

    incoming = mm(halves(s_ref[...]), halves(xpre[:LANES])) + xpre[LANES:]
    read = mm(halves(gm_ref[...]), halves(incoming), 1, 1) + hm_ref[...]
    ones = head_ones()
    center = read - head_sum(read, ones) * (1.0 / HEAD)
    spread = head_sum(center * center, ones) * (1.0 / HEAD)
    mixed_ref[...] = (center * lax.rsqrt(spread + 1e-5) * gain_ref[...]).astype(BF16)

    share = mixed_ref.shape[0] // NT
    mine = pl.ds(pl.multiple_of(tp * LANES, LANES), LANES)

    def to_row(d):
        other = lax.rem(tp + d, NT)
        part = mixed_ref.at[pl.ds(pl.multiple_of(other * share, 16), share)]
        return pltpu.make_async_remote_copy(
            part, rowmix.at[:, mine], a2a_send.at[d - 1], a2a_recv.at[d - 1],
            device_id={"y": other // NC, "c": other % NC}, device_id_type=MESH,
        )

    for d in range(1, NT):
        copy = to_row(d)
        copy.start()
        sends.append(copy)
    rowmix[:, mine] = mixed_ref[pl.ds(pl.multiple_of(tp * share, 16), share), :]
    z_round(4)
    for copy in own[3:]:
        copy.wait()
    for d in range(1, NT):
        to_row(d).wait_recv()

    width = 512
    square = jnp.zeros((share, 1), F32)
    for i in range(mid_ref.shape[1] // width):
        cols = pl.ds(i * width, width)
        proj = jnp.dot(rowmix[...], wo[:, cols], preferred_element_type=F32)
        mid = (resid[:, cols].astype(F32) + proj).astype(BF16)
        mid_ref[:, cols] = mid
        mid = mid.astype(F32)
        square += jnp.sum(mid * mid, axis=-1, keepdims=True)
    scale = lax.rsqrt(square * (1.0 / mid_ref.shape[1]) + 1e-6)
    for i in range(mid_ref.shape[1] // width):
        cols = pl.ds(i * width, width)
        rows[tp, :, cols] = (mid_ref[:, cols].astype(F32) * scale * fng_ref[:, cols]).astype(BF16)

    half = mid_ref.shape[1] // 2

    def y_rows(sem, dy, to, cols):
        ref = rows.at[lax.rem(y + dy + NY, NY) * NC + c, :, cols]
        return pltpu.make_async_remote_copy(
            ref, ref, ag_send.at[sem], ag_recv.at[sem], device_id={"y": lax.rem(y + to + NY, NY)}, device_id_type=MESH
        )

    def c_rows(sem, dy, mate):
        ref = rows.at[lax.rem(y + dy + NY, NY) * NC + (1 - c if mate else c)]
        return pltpu.make_async_remote_copy(
            ref, ref, ag_send.at[sem], ag_recv.at[sem], device_id={"c": 1 - c}, device_id_type=MESH
        )

    def go(copy):
        copy.start()
        sends.append(copy)

    every, left, right = pl.ds(0, 2 * half), pl.ds(0, half), pl.ds(half, half)
    go(y_rows(0, 0, 1, every))
    go(y_rows(1, 0, -1, every))
    go(c_rows(4, 0, False))
    x_forward(1)
    x_forward(2)
    y_rows(0, -1, 1, every).wait_recv()
    go(y_rows(2, -1, 1, left))
    go(c_rows(5, -1, False))
    y_rows(1, 1, -1, every).wait_recv()
    go(y_rows(3, 1, -1, right))
    go(c_rows(6, 1, False))
    for i in range(3):
        g_round(i, 1)
    y_rows(2, 2, 1, left).wait_recv()
    y_rows(3, 2, -1, right).wait_recv()
    go(c_rows(7, 2, False))
    for sem, dy in ((4, 0), (5, -1), (6, 1), (7, 2)):
        c_rows(sem, dy, True).wait_recv()

    x_forward(3)
    x_forward(4)
    g_round(3, 1)
    for i in range(4):
        g_round(i, 2)
    x_forward(5)
    x_forward(6)
    for i in range(4):
        g_round(i, 3)
    x_forward(7)
    x_last(0)
    for i in range(4):
        g_round(i, 4)
    for i in range(1, 8):
        x_last(i)

    tokens = NT * share
    depth, hidden = NZ * NX * wg.shape[2], wg.shape[3]
    token_rows = rows[...].reshape(tokens, depth)
    gate = jnp.dot(token_rows, wg[...].reshape(depth, hidden), preferred_element_type=F32)
    upper = jnp.dot(token_rows, wu[...].reshape(depth, hidden), preferred_element_type=F32)
    hid_ref[...] = (gate * sigmoid(gate) * upper).astype(BF16)

    def to_mate(n):
        return pltpu.make_async_remote_copy(
            sib_src.at[n], sib_buf.at[n], rs_send.at[n], rs_recv.at[n], device_id={"c": 1 - c}, device_id_type=MESH
        )

    def to_y(n, d):
        sem = COLS + n * (NY - 1) + d - 1
        return pltpu.make_async_remote_copy(
            y_src.at[n, d - 1], y_buf.at[n, d - 1], rs_send.at[sem], rs_recv.at[sem],
            device_id={"y": lax.rem(y + d, NY)}, device_id_type=MESH,
        )

    def chip_sum(n):
        to_mate(n).wait_recv()
        for d in range(NY):
            yy = lax.rem(y + d, NY)
            both = full_part[n, pl.ds(pl.multiple_of((yy * NC + c) * share, 16), share), :] + sib_buf[n, yy].astype(F32)
            if d == 0:
                own_part[n] = both
            else:
                y_src[n, d - 1] = both.astype(BF16)
                go(to_y(n, d))

    step = NZ // COLS
    for n in range(COLS):
        weights = wd[n * step : (n + 1) * step].reshape(depth // COLS, hidden)
        full_part[n] = dg(hid_ref[...], weights, 1, 1)
        for yy in range(NY):
            sib_src[n, yy] = full_part[n, pl.ds(pl.multiple_of((yy * NC + 1 - c) * share, 16), share), :].astype(BF16)
        go(to_mate(n))
        if n:
            chip_sum(n - 1)
    chip_sum(COLS - 1)
    wide = depth // COLS
    for n in range(COLS):
        acc = own_part[n]
        for d in range(1, NY):
            to_y(n, d).wait_recv()
            acc += y_buf[n, d - 1].astype(F32)
        cols = pl.ds(n * wide, wide)
        out_ref[:, cols] = (mid_ref[:, cols].astype(F32) + 0.5 * acc).astype(BF16)

    for copy in sends:
        copy.wait_send()
    for d in range(1, NZ):
        pl.when(z + d < NZ)(lambda d=d: z_state(d).wait_send())


def per_device(
    resid, queries, keys, values, decay_input_part, decay_channel_offset, decay_head_extra, correction_rate_input,
    correction_rate_offset, head_norm_gain, mixer_output_weight, feedforward_norm_gain, gate_weight, up_weight, down_weight,
):
    tokens = queries.shape[0]
    share, width = resid.shape
    shard, hidden = gate_weight.shape
    extra = jnp.repeat(decay_head_extra, HEAD, axis=1)
    vm, sem = pltpu.VMEM, pltpu.SemaphoreType.DMA
    flat = pl.BlockSpec(memory_space=pltpu.VMEM)
    there = pl.BlockSpec(memory_space=pl.ANY)
    wide = width // COLS
    weights = vm((NZ, NX, shard, hidden), BF16)
    return pl.pallas_call(
        kernel,
        name="layer",
        out_shape=jax.ShapeDtypeStruct((share, width), BF16),
        in_specs=[flat] * 10 + [there] * 5,
        out_specs=flat,
        scratch_shapes=[
            weights, weights, weights, vm(mixer_output_weight.shape, BF16), vm((share, width), BF16),
            vm((CHUNKS, LANES, LANES), F32), vm((CHUNKS, LANES, LANES), F32),
            vm((CHUNKS, LANES, LANES), F32), vm((CHUNKS, LANES, LANES), F32),
            vm((tokens, LANES), F32), vm((tokens, LANES), F32),
            vm((LANES, LANES), BF16), vm((NX - 1, LANES, LANES), BF16), vm((2 * LANES, LANES), F32),
            vm((LANES, LANES), BF16), vm((NZ - 1, LANES, LANES), BF16), vm((LANES, LANES), F32),
            vm((tokens, LANES), BF16), vm((share, NT * LANES), BF16), vm((share, width), BF16),
            vm((NT, share, width), BF16), vm((tokens, hidden), BF16),
            vm((COLS, share, wide), F32), vm((COLS, tokens, wide), F32),
            vm((COLS, NY, share, wide), BF16), vm((COLS, NY, share, wide), BF16),
            vm((COLS, NY - 1, share, wide), BF16), vm((COLS, NY - 1, share, wide), BF16),
            sem((5,)), sem((6, 8)), sem((6, 8)), sem((17, 4)), sem((17, 4)),
            sem((NX + NZ - 2,)), sem((NX + NZ - 2,)), sem((NT - 1,)), sem((NT - 1,)), sem((8,)), sem((8,)),
            sem((COLS * NY,)), sem((COLS * NY,)),
        ],
        compiler_params=pltpu.CompilerParams(collective_id=0, has_side_effects=True),
    )(
        queries, keys, values, decay_input_part, correction_rate_input,
        decay_channel_offset[None], correction_rate_offset[None], head_norm_gain[None], extra,
        feedforward_norm_gain[None], resid, mixer_output_weight, gate_weight, up_weight, down_weight.T,
    )


def solution(mesh):
    torus = Mesh(mesh.devices.reshape(NZ, NX, NY, NC), SP_TP)
    in_specs = (
        P(SP_TP, None), P(SP, TP), P(SP, TP), P(SP, TP), P(SP, TP), P(TP), P(SP, TP), P(SP, TP), P(TP), P(TP),
        P(), P(), P(SP, TP), P(SP, TP), P(TP, SP),
    )
    return jax.shard_map(per_device, mesh=torus, in_specs=in_specs, out_specs=P(SP_TP, None), check_vma=False)
```

```python
import functools

import jax
import jax.numpy as jnp
from jax import lax
from jax.experimental import pallas as pl
from jax.experimental.pallas import tpu as pltpu
from jax.sharding import Mesh
from jax.sharding import PartitionSpec as P

F32, BF16 = jnp.float32, jnp.bfloat16
MESH = pl.DeviceIdType.MESH
HEAD, LANES, CH = 64, 128, 64
NZ, NX, NY, NC = 8, 4, 4, 2
NT = NY * NC
CHUNKS = 6
GROUP = 3
COLS = ((0, 1, 2), (3, 4), (5, 6), (7,))
SP, TP, SP_TP = ("z", "x"), ("y", "c"), ("z", "x", "y", "c")


def dg(a, b, ca=1, cb=0):
    return lax.dot_general(a, b, (((ca,), (cb,)), ((), ())), preferred_element_type=F32)


def halves(x):
    hi = x.astype(BF16)
    return hi, (x - hi.astype(F32)).astype(BF16)


def mm(a, b, ca=1, cb=0):
    return dg(a[0], b[0], ca, cb) + dg(a[0], b[1], ca, cb) + dg(a[1], b[0], ca, cb)


def thirds(x):
    hi = x.astype(BF16)
    rest = x - hi.astype(F32)
    mid = rest.astype(BF16)
    return hi, mid, (rest - mid.astype(F32)).astype(BF16)


def iota(shape, dim):
    return lax.broadcasted_iota(jnp.int32, shape, dim)


def first_head(rows):
    return iota((rows, LANES), 1) < HEAD


def stacked(x):
    own = first_head(x.shape[0])
    zero = jnp.zeros_like(x)
    return jnp.concatenate([jnp.where(own, x, zero), jnp.where(own, zero, x)], axis=0)


def folded(x):
    half = x.shape[0] // 2
    return x[:half] + x[half:]


def head_ones():
    return (iota((LANES, LANES), 0) // HEAD == iota((LANES, LANES), 1) // HEAD).astype(BF16)


def head_sum(x, ones):
    hi, lo = halves(x)
    return dg(hi, ones) + dg(lo, ones)


def sigmoid(x):
    return 1.0 / (1.0 + jnp.exp(-x))


def mixer_group(first, serve, q_ref, k_ref, v_ref, dip_ref, cri_ref, dco_ref, cro_ref, extra_ref, m_ref, n_ref, r_ref, o_ref):
    ids = range(first, first + GROUP)
    ones = head_ones()
    row, col = iota((LANES, LANES), 0), iota((LANES, LANES), 1)
    eye = (row == col).astype(F32)
    low = (iota((CH, CH), 0) >= iota((CH, CH), 1)).astype(BF16)
    ends, us, bts, avs, reads, vs = [], [], [], [], [], []
    invs, offs, qks = [], [], []
    for c in ids:
        rows = pl.ds(c * CH, CH)
        q, k, v = (r[rows, :].astype(F32) for r in (q_ref, k_ref, v_ref))
        pre = dco_ref[...] + dip_ref[rows, :].astype(F32)
        log_decay = -(sigmoid(pre) * 0.6065306597126334) - extra_ref[rows, :]
        unit = k * lax.rsqrt(head_sum(k * k, ones) + 1e-6)
        b = unit * sigmoid(cro_ref[...] + cri_ref[rows, :].astype(F32))
        total = sum(dg(low, part) for part in thirds(log_decay))
        before = total - log_decay
        mid, end = total[CH // 2 - 1 : CH // 2], total[CH - 1 :]
        up, down = jnp.exp(total - mid), jnp.exp(mid - total)
        up_before = jnp.exp(before - mid)
        rest = jnp.exp(end - total)
        left = halves(jnp.concatenate([stacked(unit * up_before), stacked(q * up)], axis=0))
        right = halves(jnp.concatenate([stacked(k * down), stacked(b * down)], axis=0))
        a = mm(left, right, 1, 1)
        a_uk = jnp.where(row > col, a[:LANES, :LANES], 0.0)
        a_qk = jnp.where(row >= col, a[LANES:, :LANES], 0.0)
        a_qb = jnp.where(row >= col, a[LANES:, LANES:], 0.0)
        offs.append(a[:LANES, LANES:])
        vst = halves(stacked(v))
        av = mm(halves(jnp.concatenate([a_uk, a_qk], axis=0)), vst)
        us.append(halves(jnp.concatenate([stacked(unit * jnp.exp(before)), av[:LANES]], axis=1)))
        avs.append(av[LANES:])
        qks.append(halves(a_qb))
        reads.append(stacked(q * jnp.exp(total)))
        bts.append(halves(stacked(b * rest)))
        ends.append((jnp.exp(end), mm(vst, halves(stacked(k * rest)), 0, 0)))
    serve(first)
    size = 1
    while size < CH:
        inside = (row // (2 * size) == col // (2 * size)) & (row // size != col // size) & (row > col)
        for i in range(GROUP):
            part = jnp.where(inside, offs[i], 0.0)
            if size == 1:
                invs.append(eye - part)
            else:
                inv = halves(invs[i])
                invs[i] = invs[i] - mm(halves(mm(inv, halves(part))), inv)
        size *= 2
    serve(first + 1)
    for i, c in enumerate(ids):
        wu = mm(halves(invs[i]), us[i])
        wu2 = halves(wu)
        ro = mm(qks[i], wu2)
        r_ref[c] = reads[i] - ro[:, :LANES]
        o_ref[c] = avs[i] - ro[:, LANES:]
        mn = mm(wu2, bts[i], 0, 0)
        decay, kv = ends[i]
        m_ref[c] = jnp.where(row == col, decay, 0.0) - mn[:LANES]
        n_ref[c] = kv - mn[LANES:]


def unpacked(message):
    wide = message.astype(F32)
    return stacked(wide[:HEAD]).astype(BF16), stacked(wide[HEAD:])


def packed(trans, state):
    return jnp.concatenate([folded(trans), folded(state)], axis=0).astype(BF16)


def after(total, message):
    trans, state = unpacked(message)
    hi, lo = halves(total)
    out = dg(hi, trans) + dg(lo, trans)
    return jnp.concatenate([out[:LANES], out[LANES:] + state], axis=0)


GQ, GP, DQ, DP = 0, 1, 2, 3
PARTS = ((0, 24, 40, True), (0, 0, 24, False), (1, 24, 40, True), (1, 0, 24, False))
Z_RINGS = (0, 2, 1, 6)
X_RINGS = (0, 16, 8, 17)
DZ = (0, -1, 1, -2, 2, -3, 3, 4)
DX = (0, 1, -1, 2)
Z_ON, Z_FIRST, X_FIRST, X_ON = 0, 1, 2, 3
SCHEDULE = {
    "start": (
        (2, 1, 0, 0), (1, 0, 0, 0), (1, 1, 0, 0), (2, 0, 0, 0),
    ),
    "a2": (
        (3, 1, 0, 0), (1, 1, 1, 0), (1, 1, 2, 0),
    ),
    "a3": (
        (2, 0, 1, 0), (0, 0, 0, 1), (2, 0, 2, 0),
    ),
    "a4": (
        (0, 1, 0, 1), (3, 0, 0, 0), (1, 1, 3, 0),
    ),
    "a5": (
        (0, 1, 1, 1),
    ),
    "xsent": (
        (0, 1, 2, 1), (3, 0, 1, 0), (2, 0, 3, 0), (2, 0, 4, 0), (0, 0, 0, 2), (3, 0, 2, 0),
    ),
    "zsent": (
        (0, 1, 3, 1), (0, 1, 0, 2), (0, 1, 1, 2), (0, 1, 2, 2), (3, 0, 3, 0), (2, 0, 5, 0),
        (2, 0, 6, 0), (0, 0, 0, 3), (3, 0, 4, 0),
    ),
    "ag1": (
        (1, 2, 0, 0), (2, 2, 0, 0), (0, 1, 3, 2), (0, 1, 0, 3), (1, 3, 0, 0), (2, 3, 0, 0),
        (3, 0, 5, 0), (0, 1, 1, 3),
    ),
    "ag2": (
        (0, 1, 2, 3), (3, 0, 6, 0),
    ),
    "ag3": (
        (2, 0, 7, 0),
    ),
    "pr0": (
        (3, 2, 0, 0), (0, 2, 0, 1), (2, 2, 1, 0), (2, 2, 2, 0),
    ),
    "pr1": (
        (1, 3, 1, 0), (1, 3, 2, 0), (3, 3, 0, 0),
    ),
    "pr2": (
        (0, 1, 3, 3),
    ),
    "gu": (
        (0, 3, 0, 1), (0, 2, 0, 2), (2, 2, 3, 0), (2, 2, 4, 0), (3, 0, 7, 0), (0, 3, 1, 1),
        (0, 3, 2, 1), (3, 2, 1, 0), (0, 3, 0, 2), (3, 2, 2, 0), (1, 3, 3, 0), (0, 2, 0, 3),
        (2, 2, 5, 0), (2, 2, 6, 0), (3, 2, 3, 0), (0, 3, 1, 2), (0, 3, 2, 2), (3, 2, 4, 0),
        (0, 3, 0, 3), (0, 3, 3, 1),
    ),
    "d0": (
        (0, 3, 1, 3), (0, 3, 2, 3), (2, 2, 7, 0),
    ),
    "d1": (
        (3, 2, 5, 0), (0, 3, 3, 2), (3, 2, 6, 0),
    ),
    "d2": (
        (0, 3, 3, 3), (3, 2, 7, 0),
    ),
}


class Gather:
    def __init__(self, bufs, send_z, recv_z, send_x, recv_x, sends):
        self.bufs, self.sends, self.here, self.done = bufs, sends, set(), set()
        self.sems = {"z": (send_z, recv_z), "x": (send_x, recv_x)}
        self.place = {"z": lax.axis_index("z"), "x": lax.axis_index("x")}

    def copy(self, axis, part, i, hop, right, got):
        buf, first, rows, z_first = PARTS[part]
        sign, far = (1 if right else -1), {"z": 4, "x": 2}[axis]
        size = {"z": NZ, "x": NX}
        back = -sign * (hop if got else hop - 1)
        dz, dx = (back, DX[i]) if axis == "z" else (DZ[i], back)
        ref = self.bufs[buf].at[lax.rem(self.place["z"] + dz + NZ, NZ), lax.rem(self.place["x"] + dx + NX, NX)]
        if hop == far:
            cut = (rows // 8 + i % 2) // 2 * 8
            first, rows = (first, cut) if right else (first + cut, rows - cut)
        ref = ref.at[pl.ds(first, rows)]
        ring = (Z_RINGS if axis == "z" else X_RINGS)[part] + i
        slot = hop - 1 + (0 if right else far)
        send, recv = self.sems[axis]
        return pltpu.make_async_remote_copy(
            ref, ref, send.at[ring, slot], recv.at[ring, slot],
            device_id={axis: lax.rem(self.place[axis] + sign + size[axis], size[axis])}, device_id_type=MESH,
        )

    def send(self, axis, part, i, hop):
        for right in (True, False):
            copy = self.copy(axis, part, i, hop, right, False)
            copy.start()
            self.sends.append(copy)

    def need(self, axis, part, i, hop):
        if (axis, part, i, hop) not in self.here:
            self.here.add((axis, part, i, hop))
            for right in (True, False):
                self.copy(axis, part, i, hop, right, True).wait_recv()

    def do(self, kind, part, i, hop):
        self.done.add((kind, part, i, hop))
        z_first = PARTS[part][3]
        if kind == Z_ON:
            self.need("z", part, i, hop)
            self.send("z", part, i, hop + 1)
        elif kind == Z_FIRST:
            if not z_first and i:
                self.need("x", part, 0, 1 if i < 3 else 2)
            self.send("z", part, i, 1)
        elif kind == X_FIRST:
            if z_first and i:
                self.need("z", part, 0, (i + 1) // 2)
            self.send("x", part, i, 1)
        else:
            self.need("x", part, i, 1)
            self.send("x", part, i, 2)

    def serve(self, point):
        for task in SCHEDULE.get(point, ()):
            self.do(*task)

    def whole(self, part):
        for i in range(8 if PARTS[part][3] else 1):
            self.need("x", part, i, 1)
            self.need("x", part, i, 2)
        for i in range(1 if PARTS[part][3] else 4):
            for hop in range(1, 5):
                self.need("z", part, i, hop)

    def slab(self, q, p, i):
        hop = (i + 1) // 2
        if i:
            self.need("z", q, 0, hop)
            for j in range(4):
                self.need("z", p, j, hop)
        for part, ring in ((q, i), (p, 0)):
            self.need("x", part, ring, 1)
            self.need("x", part, ring, 2)


class Spread:
    def __init__(self, block, send_sem, recv_sem, sends):
        self.block, self.send_sem, self.recv_sem, self.sends = block, send_sem, recv_sem, sends
        self.y, self.c = lax.axis_index("y"), lax.axis_index("c")

    def along_y(self, sem, dy, up, half):
        ref = self.block(lax.rem(self.y + dy + NY, NY) * NC + self.c, half)
        return pltpu.make_async_remote_copy(
            ref, ref, self.send_sem.at[sem], self.recv_sem.at[sem],
            device_id={"y": lax.rem(self.y + (1 if up else NY - 1), NY)}, device_id_type=MESH,
        )

    def across(self, sem, dy, mine):
        ref = self.block(lax.rem(self.y + dy + NY, NY) * NC + (self.c if mine else 1 - self.c), None)
        return pltpu.make_async_remote_copy(
            ref, ref, self.send_sem.at[sem], self.recv_sem.at[sem], device_id={"c": 1 - self.c}, device_id_type=MESH
        )

    def go(self, copy):
        copy.start()
        self.sends.append(copy)

    def start(self):
        for half in (0, 1):
            self.go(self.along_y(half, 0, True, half))
            self.go(self.along_y(2 + half, 0, False, 1 - half))
        self.go(self.across(6, 0, True))

    def relay(self):
        self.along_y(0, -1, True, 0).wait_recv()
        self.go(self.along_y(4, -1, True, 0))
        self.along_y(2, 1, False, 1).wait_recv()
        self.go(self.along_y(5, 1, False, 1))

    def near(self):
        self.along_y(1, -1, True, 1).wait_recv()
        self.go(self.across(7, -1, True))
        self.along_y(3, 1, False, 0).wait_recv()
        self.go(self.across(8, 1, True))

    def far(self):
        self.along_y(4, 2, True, 0).wait_recv()
        self.along_y(5, 2, False, 1).wait_recv()
        self.go(self.across(9, 2, True))

    def finish(self):
        for sem, dy in ((6, 0), (7, -1), (8, 1), (9, 2)):
            self.across(sem, dy, False).wait_recv()


_open = []


def mark(name):
    if _open:
        _open.pop().__exit__(None, None, None)
    if name:
        _open.append(jax.named_scope(name))
        _open[-1].__enter__()


def kernel(
    q_hbm, k_hbm, v_hbm, dip_hbm, cri_hbm, dco_hbm, cro_hbm, gain_hbm, extra_t_hbm, fng_hbm,
    resid_hbm, wo_hbm, gate_hbm, up_hbm, down_hbm,
    out_ref,
    q_ref, k_ref, v_ref, dip_ref, cri_ref, dco_ref, cro_ref, gain_ref, extra_t_ref, fng_ref,
    wgu, wd, g_in, u_in, wo, resid,
    extra_ref, m_ref, n_ref, r_ref, o_ref, gm_ref, hm_ref,
    tot_ref, xbuf, xpre, zsrc, zbuf, s_ref,
    mix_all, mid_ref, rows, hid_ref,
    full_part, own_part, pair, sib_src, sib_buf, far_src, far_buf, y_src, y_buf,
    local_sem, send_z, recv_z, send_x, recv_x,
    st_send, st_recv, res_send, res_recv, ag_send, ag_recv, rs_send, rs_recv,
):
    z, x, y, c = (lax.axis_index(n) for n in SP_TP)
    tp = y * NC + c
    sends = []
    tokens, width = rows.shape
    share = tokens // NT

    def block_rows(i):
        return pl.ds(pl.multiple_of(i * share, 16), share)

    def go(copy):
        copy.start()
        sends.append(copy)

    mark("barrier")
    own = [
        pltpu.make_async_copy(src, dst, local_sem.at[i])
        for i, (src, dst) in enumerate(
            ((gate_hbm, g_in), (up_hbm, u_in), (down_hbm, wd.at[z, x]), (resid_hbm, resid.at[block_rows(tp)]),
             (extra_t_hbm, extra_t_ref), (k_hbm, k_ref), (q_hbm, q_ref), (v_hbm, v_ref), (dip_hbm, dip_ref),
             (cri_hbm, cri_ref), (dco_hbm, dco_ref), (cro_hbm, cro_ref), (gain_hbm, gain_ref), (fng_hbm, fng_ref), (wo_hbm, wo))
        )
    ]
    barrier = pltpu.get_barrier_semaphore()
    peers = [{"x": lax.rem(x + d, NX)} for d in range(1, NX)]
    peers += [{"z": lax.rem(z + d, NZ)} for d in range(1, NZ)]
    peers += [{"y": lax.rem(y + d, NY)} for d in (1, NY - 1)] + [{"c": 1 - c}]
    for peer in peers:
        pl.semaphore_signal(barrier, inc=1, device_id=peer, device_id_type=MESH)
    for copy in own:
        copy.start()
    for copy in own[:5]:
        copy.wait()
    hidden = g_in.shape[1]
    full = hidden // LANES * LANES
    wgu[z, x, :, :full] = g_in[:, :full]
    wgu[z, x, :, full : 2 * full] = u_in[:, :full]
    tail = jnp.concatenate([g_in[:, full:].astype(F32), u_in[:, full:].astype(F32)], axis=1)
    wgu[z, x, :, 2 * full :] = tail.astype(BF16)
    extra_t = jnp.concatenate([extra_t_ref[...], jnp.zeros((6, extra_t_ref.shape[1]), F32)], axis=0)
    pick = (iota((8, LANES), 0) == iota((8, LANES), 1) // HEAD).astype(BF16)
    extra_ref[...] = sum(dg(part, pick, 0, 0) for part in thirds(extra_t))
    pl.semaphore_wait(barrier, len(peers))

    g = Gather((wgu, wd), send_z, recv_z, send_x, recv_x, sends)
    g.serve("start")

    def resid_block(i, half):
        cols = pl.ds(0, width) if half is None else pl.ds(half * (width // 2), width // 2)
        return resid.at[block_rows(i), cols]

    def mix_block(i, half):
        part = pl.ds(0, tokens) if half is None else pl.ds(half * (tokens // 2), tokens // 2)
        return mix_all.at[part, pl.ds(pl.multiple_of(i * LANES, LANES), LANES)]

    res = Spread(resid_block, res_send, res_recv, sends)
    res.start()

    mix = functools.partial(
        mixer_group, serve=lambda i: g.serve(f"a{i}"), q_ref=q_ref, k_ref=k_ref, v_ref=v_ref, dip_ref=dip_ref, cri_ref=cri_ref, dco_ref=dco_ref,
        cro_ref=cro_ref, extra_ref=extra_ref, m_ref=m_ref, n_ref=n_ref, r_ref=r_ref, o_ref=o_ref,
    )
    for copy in own[5:14]:
        copy.wait()
    mark("mix0")
    mix(0)
    mark("s1")
    g.serve("a2")
    res.relay()
    mark("mix1")
    mix(GROUP)
    mark("s2")
    g.serve("a5")
    res.near()
    res.far()
    mark("prefix")

    row, col = iota((LANES, LANES), 0), iota((LANES, LANES), 1)
    start = jnp.concatenate([(row == col).astype(F32), jnp.zeros((LANES, LANES), F32)], axis=0)
    total = start
    for i in range(CHUNKS):
        split = halves(total)
        step = mm(split, halves(m_ref[i]))
        gh = mm(halves(r_ref[i]), split, 1, 1)
        rows_i = pl.ds(i * CH, CH)
        gm_ref[rows_i, :] = folded(gh[:, :LANES])
        hm_ref[rows_i, :] = folded(gh[:, LANES:] + o_ref[i])
        total = jnp.concatenate([step[:LANES], step[LANES:] + n_ref[i]], axis=0)
    tot_ref[...] = packed(total[:LANES], total[LANES:])

    def x_state(d):
        return pltpu.make_async_remote_copy(
            tot_ref, xbuf.at[d - 1], st_send.at[d - 1], st_recv.at[d - 1],
            device_id={"x": lax.rem(x + d, NX)}, device_id_type=MESH,
        )

    for d in range(1, NX):
        go(x_state(d))
    mark("s2")
    g.serve("xsent")
    mark("xstate")
    for d in range(1, NX):
        x_state(d).wait_recv()
    mark("xcomb")
    total = start
    prefix = total
    for i in range(NX):
        prefix = jnp.where(x == i, total, prefix)
        message = tot_ref[...]
        for d in range(1, NX):
            message = jnp.where(lax.rem(x - i + NX, NX) == d, xbuf[d - 1], message)
        total = after(total, message)
    xpre[...] = prefix
    zsrc[...] = packed(total[:LANES], total[LANES:])

    def z_state(d):
        return pltpu.make_async_remote_copy(
            zsrc, zbuf.at[d - 1], st_send.at[NX - 2 + d], st_recv.at[NX - 2 + d],
            device_id={"z": lax.rem(z + d, NZ)}, device_id_type=MESH,
        )

    for d in range(1, NZ):
        pl.when(z + d < NZ)(lambda d=d: z_state(d).start())
    mark("s3")
    g.serve("zsent")
    mark("zstate")
    s_ref[...] = jnp.zeros_like(s_ref)
    for d in range(NZ - 1, 0, -1):

        @pl.when(z >= d)
        def _(d=d):
            z_state(d).wait_recv()
            trans, state = unpacked(zbuf[d - 1])
            hi, lo = halves(s_ref[...])
            s_ref[...] = dg(hi, trans) + dg(lo, trans) + state

    mark("read")
    incoming = mm(halves(s_ref[...]), halves(xpre[:LANES])) + xpre[LANES:]
    read = mm(halves(gm_ref[...]), halves(incoming), 1, 1) + hm_ref[...]
    ones = head_ones()
    center = read - head_sum(read, ones) * (1.0 / HEAD)
    spread = head_sum(center * center, ones) * (1.0 / HEAD)
    mine = pl.ds(pl.multiple_of(tp * LANES, LANES), LANES)
    mix_all[:, mine] = (center * lax.rsqrt(spread + 1e-5) * gain_ref[...]).astype(BF16)
    mixed = Spread(mix_block, ag_send, ag_recv, sends)
    mixed.start()
    mark("ag1")
    g.serve("ag1")
    mark("ag1w")
    mixed.relay()
    mark("ag2")
    g.serve("ag2")
    mark("ag2w")
    mixed.near()
    mixed.far()
    mark("ag3")
    g.serve("ag3")
    mark("ag3w")
    own[14].wait()
    res.finish()
    mixed.finish()

    tile = 512
    square = jnp.zeros((tokens, 1), F32)
    for i in range(width // tile):
        mark(f"pr{i}")
        cols = pl.ds(i * tile, tile)
        proj = jnp.dot(mix_all[...], wo[:, cols], preferred_element_type=F32)
        mid = (resid[:, cols].astype(F32) + proj).astype(BF16)
        mid_ref[:, cols] = mid
        mid = mid.astype(F32)
        square += jnp.sum(mid * mid, axis=-1, keepdims=True)
        mark(f"sp{i}")
        g.serve(f"pr{i}")
    mark("norm")
    scale = lax.rsqrt(square * (1.0 / width) + 1e-6)
    for i in range(width // tile):
        cols = pl.ds(i * tile, tile)
        rows[:, cols] = (mid_ref[:, cols].astype(F32) * scale * fng_ref[:, cols]).astype(BF16)
    mark("gu")
    g.serve("gu")
    g.whole(GQ)
    g.whole(GP)

    mark("gateup")
    both = jnp.dot(rows[...], wgu[...].reshape(width, 2 * hidden), preferred_element_type=F32)

    def gated(gate, upper):
        return (gate * sigmoid(gate) * upper).astype(BF16)

    rest = hidden - full
    hid_ref[:, :full] = gated(both[:, :full], both[:, full : 2 * full])
    hid_ref[:, full:] = gated(both[:, 2 * full : 2 * full + rest], both[:, 2 * full + rest :])

    slab = width // NZ

    def wide(n):
        return len(COLS[n]) * slab

    def to_mate(n):
        cols = pl.ds(0, wide(n))
        return pltpu.make_async_remote_copy(
            sib_src.at[n, :, :, cols], sib_buf.at[n, :, :, cols], rs_send.at[n, 0], rs_recv.at[n, 0],
            device_id={"c": 1 - c}, device_id_type=MESH,
        )

    def to_y(n, kind, up):
        src, dst = (far_src, far_buf) if kind == 0 else (y_src, y_buf)
        cols = pl.ds(0, wide(n) // 2 if kind == 0 else wide(n))
        k = 0 if up else 1
        sem = 1 + 2 * kind + k
        return pltpu.make_async_remote_copy(
            src.at[n, k, :, cols], dst.at[n, k, :, cols], rs_send.at[n, sem], rs_recv.at[n, sem],
            device_id={"y": lax.rem(y + (1 if up else NY - 1), NY)}, device_id_type=MESH,
        )

    def place(i):
        return lax.rem(z + DZ[i] + NZ, NZ)

    def product(n):
        for k, i in enumerate(COLS[n]):
            full_part[n, :, k * slab : (k + 1) * slab] = dg(hid_ref[...], wd[place(i)].reshape(slab, hidden), 1, 1)
        for yy in range(NY):
            sib_src[n, yy, :, : wide(n)] = full_part[n, block_rows(yy * NC + 1 - c), : wide(n)].astype(BF16)
        go(to_mate(n))

    def chip_sum(n):
        to_mate(n).wait_recv()
        w, h = wide(n), wide(n) // 2

        def of(d):
            yy = lax.rem(y + d, NY)
            return full_part[n, block_rows(yy * NC + c), :w] + sib_buf[n, yy, :, :w].astype(F32)

        far = of(2).astype(BF16)
        far_src[n, 0, :, :h] = far[:, :h]
        far_src[n, 1, :, :h] = far[:, h:]
        go(to_y(n, 0, True))
        go(to_y(n, 0, False))
        own_part[n, :, :w] = of(0)
        pair[n, 0, :, :w] = of(1)
        pair[n, 1, :, :w] = of(3)

    def ring_sum(n):
        w, h = wide(n), wide(n) // 2
        to_y(n, 0, True).wait_recv()
        y_src[n, 0, :, :h] = (pair[n, 0, :, :h] + far_buf[n, 0, :, :h].astype(F32)).astype(BF16)
        y_src[n, 0, :, h:w] = pair[n, 0, :, h:w].astype(BF16)
        go(to_y(n, 1, True))
        to_y(n, 0, False).wait_recv()
        y_src[n, 1, :, :h] = pair[n, 1, :, :h].astype(BF16)
        y_src[n, 1, :, h:w] = (pair[n, 1, :, h:w] + far_buf[n, 1, :, :h].astype(F32)).astype(BF16)
        go(to_y(n, 1, False))

    def finish(n):
        for up in (True, False):
            to_y(n, 1, up).wait_recv()
        for k, i in enumerate(COLS[n]):
            at = slice(k * slab, (k + 1) * slab)
            acc = own_part[n, :, at] + y_buf[n, 0, :, at].astype(F32) + y_buf[n, 1, :, at].astype(F32)
            cols = pl.ds(pl.multiple_of(place(i) * slab, slab), slab)
            out_ref[:, cols] = (mid_ref[block_rows(tp), cols].astype(F32) + 0.5 * acc).astype(BF16)

    for n in range(len(COLS)):
        mark(f"d{n}")
        g.serve(f"d{n}")
        if n > 0:
            chip_sum(n - 1)
        if n > 1:
            ring_sum(n - 2)
        mark(f"w{n}")
        for i in COLS[n]:
            g.slab(DQ, DP, i)
        mark(f"p{n}")
        product(n)
    last = len(COLS) - 1
    mark("cs3")
    chip_sum(last)
    mark("rs2")
    ring_sum(last - 1)
    mark("fin01")
    for n in range(last - 1):
        finish(n)
    mark("rs3")
    ring_sum(last)
    mark("fin2")
    finish(last - 1)
    mark("fin3")
    finish(last)
    mark("sendwait")
    for copy in sends:
        copy.wait_send()
    for d in range(1, NZ):
        pl.when(z + d < NZ)(lambda d=d: z_state(d).wait_send())
    mark(None)


def per_device(
    resid, queries, keys, values, decay_input_part, decay_channel_offset, decay_head_extra, correction_rate_input,
    correction_rate_offset, head_norm_gain, mixer_output_weight, feedforward_norm_gain, gate_weight, up_weight, down_weight,
):
    tokens = queries.shape[0]
    share, width = resid.shape
    shard, hidden = gate_weight.shape
    vm, sem = pltpu.VMEM, pltpu.SemaphoreType.DMA
    flat = pl.BlockSpec(memory_space=pltpu.VMEM)
    there = pl.BlockSpec(memory_space=pl.ANY)
    slab = width // NZ
    parts, wide = len(COLS), max(map(len, COLS)) * slab
    return pl.pallas_call(
        kernel,
        name="layer",
        out_shape=pltpu.VMEM((share, width), BF16),
        in_specs=[there] * 15,
        out_specs=flat,
        scratch_shapes=[
            *[vm((tokens, LANES), BF16)] * 5, *[vm((1, LANES), F32)] * 3, vm((LANES // HEAD, tokens), F32), vm((1, width), F32),
            vm((NZ, NX, shard, 2 * hidden), BF16), vm((NZ, NX, shard, hidden), BF16),
            vm((shard, hidden), BF16), vm((shard, hidden), BF16),
            vm(mixer_output_weight.shape, BF16), vm((tokens, width), BF16),
            vm((tokens, LANES), F32),
            vm((CHUNKS, LANES, LANES), F32), vm((CHUNKS, LANES, LANES), F32),
            vm((CHUNKS, LANES, LANES), F32), vm((CHUNKS, LANES, LANES), F32),
            vm((tokens, LANES), F32), vm((tokens, LANES), F32),
            vm((LANES, LANES), BF16), vm((NX - 1, LANES, LANES), BF16), vm((2 * LANES, LANES), F32),
            vm((LANES, LANES), BF16), vm((NZ - 1, LANES, LANES), BF16), vm((LANES, LANES), F32),
            vm((tokens, NT * LANES), BF16), vm((tokens, width), BF16), vm((tokens, width), BF16), vm((tokens, hidden), BF16),
            vm((parts, tokens, wide), F32), vm((parts, share, wide), F32), vm((parts, 2, share, wide), F32),
            vm((parts, NY, share, wide), BF16), vm((parts, NY, share, wide), BF16),
            vm((parts, 2, share, wide // 2), BF16), vm((parts, 2, share, wide // 2), BF16),
            vm((parts, 2, share, wide), BF16), vm((parts, 2, share, wide), BF16),
            sem((15,)), sem((10, 8)), sem((10, 8)), sem((18, 4)), sem((18, 4)),
            sem((NX + NZ - 2,)), sem((NX + NZ - 2,)), sem((10,)), sem((10,)), sem((10,)), sem((10,)),
            sem((parts, 5)), sem((parts, 5)),
        ],
        compiler_params=pltpu.CompilerParams(collective_id=0, has_side_effects=True),
    )(
        queries, keys, values, decay_input_part, correction_rate_input,
        decay_channel_offset[None], correction_rate_offset[None], head_norm_gain[None], decay_head_extra.T,
        feedforward_norm_gain[None], resid, mixer_output_weight, gate_weight, up_weight, down_weight.T,
    )


def solution(mesh):
    torus = Mesh(mesh.devices.reshape(NZ, NX, NY, NC), SP_TP)
    in_specs = (
        P(SP_TP, None), P(SP, TP), P(SP, TP), P(SP, TP), P(SP, TP), P(TP), P(SP, TP), P(SP, TP), P(TP), P(TP),
        P(), P(), P(SP, TP), P(SP, TP), P(TP, SP),
    )
    return jax.shard_map(per_device, mesh=torus, in_specs=in_specs, out_specs=P(SP_TP, None), check_vma=False)
```

```python
import functools

import jax
import jax.numpy as jnp
from jax import lax
from jax.experimental import pallas as pl
from jax.experimental.pallas import tpu as pltpu
from jax.sharding import Mesh
from jax.sharding import PartitionSpec as P

F32, BF16 = jnp.float32, jnp.bfloat16
MESH = pl.DeviceIdType.MESH
HEAD, LANES, CH = 64, 128, 64
NZ, NX, NY, NC = 8, 4, 4, 2
NT = NY * NC
ZG = NZ // 2
CHUNKS = 6
GROUP = 3
COLS = ((0, 1, 2), (3, 4), (5, 6), (7,))
SP, TP, SP_TP = ("z", "x"), ("y", "c"), ("z", "x", "y", "c")


def dg(a, b, ca=1, cb=0):
    return lax.dot_general(a, b, (((ca,), (cb,)), ((), ())), preferred_element_type=F32)


def halves(x):
    hi = x.astype(BF16)
    return hi, (x - hi.astype(F32)).astype(BF16)


def mm(a, b, ca=1, cb=0):
    return dg(a[0], b[0], ca, cb) + dg(a[0], b[1], ca, cb) + dg(a[1], b[0], ca, cb)


def thirds(x):
    hi = x.astype(BF16)
    rest = x - hi.astype(F32)
    mid = rest.astype(BF16)
    return hi, mid, (rest - mid.astype(F32)).astype(BF16)


def iota(shape, dim):
    return lax.broadcasted_iota(jnp.int32, shape, dim)


def first_head(rows):
    return iota((rows, LANES), 1) < HEAD


def stacked(x):
    own = first_head(x.shape[0])
    zero = jnp.zeros_like(x)
    return jnp.concatenate([jnp.where(own, x, zero), jnp.where(own, zero, x)], axis=0)


def folded(x):
    half = x.shape[0] // 2
    return x[:half] + x[half:]


def head_ones():
    return (iota((LANES, LANES), 0) // HEAD == iota((LANES, LANES), 1) // HEAD).astype(BF16)


def head_sum(x, ones):
    hi, lo = halves(x)
    return dg(hi, ones) + dg(lo, ones)


def sigmoid(x):
    return 1.0 / (1.0 + jnp.exp(-x))


def mixer_group(first, serve, q_ref, k_ref, v_ref, dip_ref, cri_ref, dco_ref, cro_ref, extra_ref, m_ref, n_ref, r_ref, o_ref):
    ids = range(first, first + GROUP)
    ones = head_ones()
    row, col = iota((LANES, LANES), 0), iota((LANES, LANES), 1)
    eye = (row == col).astype(F32)
    low = (iota((CH, CH), 0) >= iota((CH, CH), 1)).astype(BF16)
    ends, us, bts, avs, reads, vs = [], [], [], [], [], []
    invs, offs, qks = [], [], []
    for c in ids:
        rows = pl.ds(c * CH, CH)
        q, k, v = (r[rows, :].astype(F32) for r in (q_ref, k_ref, v_ref))
        pre = dco_ref[...] + dip_ref[rows, :].astype(F32)
        log_decay = -(sigmoid(pre) * 0.6065306597126334) - extra_ref[rows, :]
        unit = k * lax.rsqrt(head_sum(k * k, ones) + 1e-6)
        b = unit * sigmoid(cro_ref[...] + cri_ref[rows, :].astype(F32))
        total = sum(dg(low, part) for part in thirds(log_decay))
        before = total - log_decay
        mid, end = total[CH // 2 - 1 : CH // 2], total[CH - 1 :]
        up, down = jnp.exp(total - mid), jnp.exp(mid - total)
        up_before = jnp.exp(before - mid)
        rest = jnp.exp(end - total)
        left = halves(jnp.concatenate([stacked(unit * up_before), stacked(q * up)], axis=0))
        right = halves(jnp.concatenate([stacked(k * down), stacked(b * down)], axis=0))
        a = mm(left, right, 1, 1)
        a_uk = jnp.where(row > col, a[:LANES, :LANES], 0.0)
        a_qk = jnp.where(row >= col, a[LANES:, :LANES], 0.0)
        a_qb = jnp.where(row >= col, a[LANES:, LANES:], 0.0)
        offs.append(a[:LANES, LANES:])
        vst = halves(stacked(v))
        av = mm(halves(jnp.concatenate([a_uk, a_qk], axis=0)), vst)
        us.append(halves(jnp.concatenate([stacked(unit * jnp.exp(before)), av[:LANES]], axis=1)))
        avs.append(av[LANES:])
        qks.append(halves(a_qb))
        reads.append(stacked(q * jnp.exp(total)))
        bts.append(halves(stacked(b * rest)))
        ends.append((jnp.exp(end), mm(vst, halves(stacked(k * rest)), 0, 0)))
    serve(first)
    size = 1
    while size < CH:
        inside = (row // (2 * size) == col // (2 * size)) & (row // size != col // size) & (row > col)
        for i in range(GROUP):
            part = jnp.where(inside, offs[i], 0.0)
            if size == 1:
                invs.append(eye - part)
            else:
                inv = halves(invs[i])
                invs[i] = invs[i] - mm(halves(mm(inv, halves(part))), inv)
        size *= 2
    serve(first + 1)
    for i, c in enumerate(ids):
        wu = mm(halves(invs[i]), us[i])
        wu2 = halves(wu)
        ro = mm(qks[i], wu2)
        r_ref[c] = reads[i] - ro[:, :LANES]
        o_ref[c] = avs[i] - ro[:, LANES:]
        mn = mm(wu2, bts[i], 0, 0)
        decay, kv = ends[i]
        m_ref[c] = jnp.where(row == col, decay, 0.0) - mn[:LANES]
        n_ref[c] = kv - mn[LANES:]


def unpacked(message):
    wide = message.astype(F32)
    return stacked(wide[:HEAD]).astype(BF16), stacked(wide[HEAD:])


def packed(trans, state):
    return jnp.concatenate([folded(trans), folded(state)], axis=0).astype(BF16)


def after(total, message):
    trans, state = unpacked(message)
    hi, lo = halves(total)
    out = dg(hi, trans) + dg(lo, trans)
    return jnp.concatenate([out[:LANES], out[LANES:] + state], axis=0)


GQ, GP, DQ, DP = 0, 1, 2, 3
PARTS = ((0, 24, 40, True), (0, 0, 24, False), (1, 32, 32, True), (1, 0, 32, False))
Z_RINGS = (0, 2, 1, 6)
X_RINGS = (0, 16, 8, 17)
DZ = (0, -1, 1, -2, 2, -3, 3, 4)
DX = (0, 1, -1, 2)
Z_ON, Z_FIRST, X_FIRST, X_ON = 0, 1, 2, 3
SCHEDULE = {
    "start": (
        (1, 2, 0, 0), (1, 3, 0, 0), (2, 1, 0, 0), (2, 3, 0, 0), (1, 0, 0, 0), (1, 1, 0, 0),
        (2, 0, 0, 0),
    ),
    "a1": (
        (2, 2, 0, 0),
    ),
    "a2": (
        (0, 2, 0, 1), (1, 1, 1, 0), (3, 1, 0, 0), (1, 1, 2, 0), (2, 2, 1, 0),
    ),
    "a3": (
        (3, 3, 0, 0), (0, 0, 0, 1), (2, 0, 1, 0),
    ),
    "a4": (
        (0, 1, 0, 1),
    ),
    "xsent": (
        (3, 0, 0, 0), (1, 1, 3, 0), (2, 0, 2, 0), (0, 1, 1, 1), (3, 0, 1, 0), (2, 0, 3, 0),
        (2, 0, 4, 0),
    ),
    "zsent": (
        (0, 0, 0, 2), (0, 1, 2, 1), (0, 1, 0, 2), (3, 0, 2, 0), (2, 2, 2, 0),
    ),
    "z2sent": (
        (3, 0, 3, 0), (1, 3, 1, 0), (0, 0, 0, 3), (2, 0, 5, 0), (2, 0, 6, 0), (0, 1, 3, 1),
        (0, 1, 1, 2), (0, 1, 2, 2), (3, 0, 4, 0), (0, 1, 0, 3),
    ),
    "ag1": (
        (2, 0, 7, 0), (1, 3, 2, 0), (3, 0, 5, 0), (0, 1, 3, 2), (0, 1, 1, 3),
    ),
    "ag2": (
        (3, 0, 6, 0), (1, 3, 3, 0), (0, 1, 2, 3), (2, 2, 3, 0), (0, 2, 0, 2),
    ),
    "ag3": (
        (3, 2, 0, 0), (0, 3, 0, 1), (2, 2, 4, 0),
    ),
    "pr0": (
        (3, 0, 7, 0), (0, 3, 1, 1), (0, 1, 3, 3),
    ),
    "pr2": (
        (0, 3, 2, 1), (3, 2, 1, 0),
    ),
    "pr3": (
        (3, 2, 2, 0), (0, 3, 3, 1),
    ),
    "gu": (
        (2, 2, 5, 0), (3, 2, 3, 0), (0, 2, 0, 3), (2, 2, 6, 0), (0, 3, 0, 2), (3, 2, 4, 0),
        (0, 3, 1, 2),
    ),
    "d0": (
        (0, 3, 2, 2), (0, 3, 3, 2), (3, 2, 5, 0), (2, 2, 7, 0),
    ),
    "d1": (
        (3, 2, 6, 0), (0, 3, 0, 3), (0, 3, 1, 3),
    ),
    "d2": (
        (0, 3, 2, 3), (3, 2, 7, 0), (0, 3, 3, 3),
    ),
}


class Gather:
    def __init__(self, bufs, send_z, recv_z, send_x, recv_x, sends):
        self.bufs, self.sends, self.here, self.done = bufs, sends, set(), set()
        self.sems = {"z": (send_z, recv_z), "x": (send_x, recv_x)}
        self.place = {"z": lax.axis_index("z"), "x": lax.axis_index("x")}

    def copy(self, axis, part, i, hop, right, got):
        buf, first, rows, z_first = PARTS[part]
        sign, far = (1 if right else -1), {"z": 4, "x": 2}[axis]
        size = {"z": NZ, "x": NX}
        back = -sign * (hop if got else hop - 1)
        dz, dx = (back, DX[i]) if axis == "z" else (DZ[i], back)
        ref = self.bufs[buf].at[lax.rem(self.place["z"] + dz + NZ, NZ), lax.rem(self.place["x"] + dx + NX, NX)]
        if hop == far:
            cut = (rows // 8 + i % 2) // 2 * 8
            first, rows = (first, cut) if right else (first + cut, rows - cut)
        ref = ref.at[pl.ds(first, rows)]
        ring = (Z_RINGS if axis == "z" else X_RINGS)[part] + i
        slot = hop - 1 + (0 if right else far)
        send, recv = self.sems[axis]
        return pltpu.make_async_remote_copy(
            ref, ref, send.at[ring, slot], recv.at[ring, slot],
            device_id={axis: lax.rem(self.place[axis] + sign + size[axis], size[axis])}, device_id_type=MESH,
        )

    def send(self, axis, part, i, hop):
        for right in (True, False):
            copy = self.copy(axis, part, i, hop, right, False)
            copy.start()
            self.sends.append(copy)

    def need(self, axis, part, i, hop):
        if (axis, part, i, hop) not in self.here:
            self.here.add((axis, part, i, hop))
            for right in (True, False):
                self.copy(axis, part, i, hop, right, True).wait_recv()

    def do(self, kind, part, i, hop):
        self.done.add((kind, part, i, hop))
        z_first = PARTS[part][3]
        if kind == Z_ON:
            self.need("z", part, i, hop)
            self.send("z", part, i, hop + 1)
        elif kind == Z_FIRST:
            if not z_first and i:
                self.need("x", part, 0, 1 if i < 3 else 2)
            self.send("z", part, i, 1)
        elif kind == X_FIRST:
            if z_first and i:
                self.need("z", part, 0, (i + 1) // 2)
            self.send("x", part, i, 1)
        else:
            self.need("x", part, i, 1)
            self.send("x", part, i, 2)

    def serve(self, point):
        for task in SCHEDULE.get(point, ()):
            self.do(*task)

    def whole(self, part):
        for i in range(8 if PARTS[part][3] else 1):
            self.need("x", part, i, 1)
            self.need("x", part, i, 2)
        for i in range(1 if PARTS[part][3] else 4):
            for hop in range(1, 5):
                self.need("z", part, i, hop)

    def slab(self, q, p, i):
        hop = (i + 1) // 2
        if i:
            self.need("z", q, 0, hop)
            for j in range(4):
                self.need("z", p, j, hop)
        for part, ring in ((q, i), (p, 0)):
            self.need("x", part, ring, 1)
            self.need("x", part, ring, 2)


class Spread:
    def __init__(self, block, send_sem, recv_sem, sends):
        self.block, self.send_sem, self.recv_sem, self.sends = block, send_sem, recv_sem, sends
        self.y, self.c = lax.axis_index("y"), lax.axis_index("c")

    def along_y(self, sem, dy, up, half):
        ref = self.block(lax.rem(self.y + dy + NY, NY) * NC + self.c, half)
        return pltpu.make_async_remote_copy(
            ref, ref, self.send_sem.at[sem], self.recv_sem.at[sem],
            device_id={"y": lax.rem(self.y + (1 if up else NY - 1), NY)}, device_id_type=MESH,
        )

    def across(self, sem, dy, mine):
        ref = self.block(lax.rem(self.y + dy + NY, NY) * NC + (self.c if mine else 1 - self.c), None)
        return pltpu.make_async_remote_copy(
            ref, ref, self.send_sem.at[sem], self.recv_sem.at[sem], device_id={"c": 1 - self.c}, device_id_type=MESH
        )

    def go(self, copy):
        copy.start()
        self.sends.append(copy)

    def start(self):
        for half in (0, 1):
            self.go(self.along_y(half, 0, True, half))
            self.go(self.along_y(2 + half, 0, False, 1 - half))
        self.go(self.across(6, 0, True))

    def relay(self):
        self.along_y(0, -1, True, 0).wait_recv()
        self.go(self.along_y(4, -1, True, 0))
        self.along_y(2, 1, False, 1).wait_recv()
        self.go(self.along_y(5, 1, False, 1))

    def near(self):
        self.along_y(1, -1, True, 1).wait_recv()
        self.go(self.across(7, -1, True))
        self.along_y(3, 1, False, 0).wait_recv()
        self.go(self.across(8, 1, True))

    def far(self):
        self.along_y(4, 2, True, 0).wait_recv()
        self.along_y(5, 2, False, 1).wait_recv()
        self.go(self.across(9, 2, True))

    def finish(self):
        for sem, dy in ((6, 0), (7, -1), (8, 1), (9, 2)):
            self.across(sem, dy, False).wait_recv()


_open = []


def mark(name):
    if _open:
        _open.pop().__exit__(None, None, None)
    if name:
        _open.append(jax.named_scope(name))
        _open[-1].__enter__()


def kernel(
    q_hbm, k_hbm, v_hbm, dip_hbm, cri_hbm, dco_hbm, cro_hbm, gain_hbm, extra_t_hbm, fng_hbm,
    resid_hbm, wo_hbm, gate_hbm, up_hbm, down_hbm,
    out_ref,
    q_ref, k_ref, v_ref, dip_ref, cri_ref, dco_ref, cro_ref, gain_ref, extra_t_ref, fng_ref,
    wgu, wd, g_in, u_in, wo, resid,
    extra_ref, m_ref, n_ref, r_ref, o_ref, gm_ref, hm_ref,
    tot_ref, xbuf, xpre, zsrc, zbuf, s_ref, z2src, z2buf,
    mix_all, mid_ref, rows, hid_ref,
    full_part, own_part, pair, sib_src, sib_buf, far_src, far_buf, y_src, y_buf,
    local_sem, send_z, recv_z, send_x, recv_x,
    st_send, st_recv, res_send, res_recv, ag_send, ag_recv, rs_send, rs_recv,
):
    z, x, y, c = (lax.axis_index(n) for n in SP_TP)
    tp = y * NC + c
    sends = []
    tokens, width = rows.shape
    share = tokens // NT

    def block_rows(i):
        return pl.ds(pl.multiple_of(i * share, 16), share)

    def go(copy):
        copy.start()
        sends.append(copy)

    mark("barrier")
    own = [
        pltpu.make_async_copy(src, dst, local_sem.at[i])
        for i, (src, dst) in enumerate(
            ((gate_hbm, g_in), (up_hbm, u_in), (down_hbm, wd.at[z, x]), (resid_hbm, resid.at[block_rows(tp)]),
             (extra_t_hbm, extra_t_ref), (k_hbm, k_ref), (q_hbm, q_ref), (v_hbm, v_ref), (dip_hbm, dip_ref),
             (cri_hbm, cri_ref), (dco_hbm, dco_ref), (cro_hbm, cro_ref), (gain_hbm, gain_ref), (fng_hbm, fng_ref), (wo_hbm, wo))
        )
    ]
    barrier = pltpu.get_barrier_semaphore()
    peers = [{"x": lax.rem(x + d, NX)} for d in range(1, NX)]
    peers += [{"z": lax.rem(z + d, NZ)} for d in range(1, NZ)]
    peers += [{"y": lax.rem(y + d, NY)} for d in (1, NY - 1)] + [{"c": 1 - c}]
    for peer in peers:
        pl.semaphore_signal(barrier, inc=1, device_id=peer, device_id_type=MESH)
    for copy in own:
        copy.start()
    for copy in own[:5]:
        copy.wait()
    hidden = g_in.shape[1]
    full = hidden // LANES * LANES
    wgu[z, x, :, :full] = g_in[:, :full]
    wgu[z, x, :, full : 2 * full] = u_in[:, :full]
    tail = jnp.concatenate([g_in[:, full:].astype(F32), u_in[:, full:].astype(F32)], axis=1)
    wgu[z, x, :, 2 * full :] = tail.astype(BF16)
    extra_t = jnp.concatenate([extra_t_ref[...], jnp.zeros((6, extra_t_ref.shape[1]), F32)], axis=0)
    pick = (iota((8, LANES), 0) == iota((8, LANES), 1) // HEAD).astype(BF16)
    extra_ref[...] = sum(dg(part, pick, 0, 0) for part in thirds(extra_t))
    pl.semaphore_wait(barrier, len(peers))

    g = Gather((wgu, wd), send_z, recv_z, send_x, recv_x, sends)
    g.serve("start")

    def resid_block(i, half):
        cols = pl.ds(0, width) if half is None else pl.ds(half * (width // 2), width // 2)
        return resid.at[block_rows(i), cols]

    def mix_block(i, half):
        part = pl.ds(0, tokens) if half is None else pl.ds(half * (tokens // 2), tokens // 2)
        return mix_all.at[part, pl.ds(pl.multiple_of(i * LANES, LANES), LANES)]

    res = Spread(resid_block, res_send, res_recv, sends)
    res.start()

    mix = functools.partial(
        mixer_group, serve=lambda i: g.serve(f"a{i}"), q_ref=q_ref, k_ref=k_ref, v_ref=v_ref, dip_ref=dip_ref, cri_ref=cri_ref, dco_ref=dco_ref,
        cro_ref=cro_ref, extra_ref=extra_ref, m_ref=m_ref, n_ref=n_ref, r_ref=r_ref, o_ref=o_ref,
    )
    for copy in own[5:14]:
        copy.wait()
    mark("mix0")
    mix(0)
    mark("s1")
    g.serve("a2")
    res.relay()
    mark("mix1")
    mix(GROUP)
    mark("s2")
    g.serve("a5")
    res.near()
    res.far()
    mark("prefix")

    row, col = iota((LANES, LANES), 0), iota((LANES, LANES), 1)
    start = jnp.concatenate([(row == col).astype(F32), jnp.zeros((LANES, LANES), F32)], axis=0)
    total = start
    for i in range(CHUNKS):
        split = halves(total)
        step = mm(split, halves(m_ref[i]))
        gh = mm(halves(r_ref[i]), split, 1, 1)
        rows_i = pl.ds(i * CH, CH)
        gm_ref[rows_i, :] = folded(gh[:, :LANES])
        hm_ref[rows_i, :] = folded(gh[:, LANES:] + o_ref[i])
        total = jnp.concatenate([step[:LANES], step[LANES:] + n_ref[i]], axis=0)
    tot_ref[...] = packed(total[:LANES], total[LANES:])

    def x_state(d):
        return pltpu.make_async_remote_copy(
            tot_ref, xbuf.at[d - 1], st_send.at[d - 1], st_recv.at[d - 1],
            device_id={"x": lax.rem(x + d, NX)}, device_id_type=MESH,
        )

    for d in range(1, NX):
        go(x_state(d))
    mark("s2")
    g.serve("xsent")
    mark("xstate")
    for d in range(1, NX):
        x_state(d).wait_recv()
    mark("xcomb")
    total = start
    prefix = total
    for i in range(NX):
        prefix = jnp.where(x == i, total, prefix)
        message = tot_ref[...]
        for d in range(1, NX):
            message = jnp.where(lax.rem(x - i + NX, NX) == d, xbuf[d - 1], message)
        total = after(total, message)
    xpre[...] = prefix
    zsrc[...] = packed(total[:LANES], total[LANES:])

    place_z, far_half = lax.rem(z, ZG), z >= ZG

    def z_state(d):
        return pltpu.make_async_remote_copy(
            zsrc, zbuf.at[d - 1], st_send.at[NX - 2 + d], st_recv.at[NX - 2 + d],
            device_id={"z": lax.rem(z + d, NZ)}, device_id_type=MESH,
        )

    def z_half(d):
        return pltpu.make_async_remote_copy(
            z2src, z2buf, st_send.at[NX + ZG - 3 + d], st_recv.at[NX + ZG - 2],
            device_id={"z": lax.rem(z + d, NZ)}, device_id_type=MESH,
        )

    for d in range(1, ZG):
        pl.when(place_z + d < ZG)(lambda d=d: z_state(d).start())
    mark("s3")
    g.serve("zsent")
    mark("zstate")
    s_ref[...] = start
    for d in range(ZG - 1, 0, -1):

        @pl.when(place_z >= d)
        def _(d=d):
            z_state(d).wait_recv()
            s_ref[...] = after(s_ref[...], zbuf[d - 1])

    @pl.when(z == ZG - 1)
    def _():
        z2src[...] = folded(after(s_ref[...], zsrc[...])[LANES:]).astype(BF16)
        for d in range(1, ZG + 1):
            z_half(d).start()

    mark("s3b")
    g.serve("z2sent")
    mark("zhalf")

    @pl.when(far_half)
    def _():
        z_half(1).wait_recv()
        s_ref[LANES:] += mm(halves(stacked(z2buf[...].astype(F32))), halves(s_ref[:LANES]))

    mark("read")
    incoming = mm(halves(s_ref[LANES:]), halves(xpre[:LANES])) + xpre[LANES:]
    read = mm(halves(gm_ref[...]), halves(incoming), 1, 1) + hm_ref[...]
    ones = head_ones()
    center = read - head_sum(read, ones) * (1.0 / HEAD)
    spread = head_sum(center * center, ones) * (1.0 / HEAD)
    mine = pl.ds(pl.multiple_of(tp * LANES, LANES), LANES)
    mix_all[:, mine] = (center * lax.rsqrt(spread + 1e-5) * gain_ref[...]).astype(BF16)
    mixed = Spread(mix_block, ag_send, ag_recv, sends)
    mixed.start()
    mark("ag1")
    g.serve("ag1")
    mark("ag1w")
    mixed.relay()
    mark("ag2")
    g.serve("ag2")
    mark("ag2w")
    mixed.near()
    mixed.far()
    mark("ag3")
    g.serve("ag3")
    mark("ag3w")
    own[14].wait()
    res.finish()
    mixed.finish()

    tile = 512
    square = jnp.zeros((tokens, 1), F32)
    for i in range(width // tile):
        mark(f"pr{i}")
        cols = pl.ds(i * tile, tile)
        proj = jnp.dot(mix_all[...], wo[:, cols], preferred_element_type=F32)
        mid = (resid[:, cols].astype(F32) + proj).astype(BF16)
        mid_ref[:, cols] = mid
        mid = mid.astype(F32)
        square += jnp.sum(mid * mid, axis=-1, keepdims=True)
        mark(f"sp{i}")
        g.serve(f"pr{i}")
    mark("norm")
    scale = lax.rsqrt(square * (1.0 / width) + 1e-6)
    for i in range(width // tile):
        cols = pl.ds(i * tile, tile)
        rows[:, cols] = (mid_ref[:, cols].astype(F32) * scale * fng_ref[:, cols]).astype(BF16)
    mark("gu")
    g.serve("gu")
    g.whole(GQ)
    g.whole(GP)

    mark("gateup")
    both = jnp.dot(rows[...], wgu[...].reshape(width, 2 * hidden), preferred_element_type=F32)

    def gated(gate, upper):
        return (gate * sigmoid(gate) * upper).astype(BF16)

    rest = hidden - full
    hid_ref[:, :full] = gated(both[:, :full], both[:, full : 2 * full])
    hid_ref[:, full:] = gated(both[:, 2 * full : 2 * full + rest], both[:, 2 * full + rest :])

    slab = width // NZ

    def wide(n):
        return len(COLS[n]) * slab

    def to_mate(n):
        cols = pl.ds(0, wide(n))
        return pltpu.make_async_remote_copy(
            sib_src.at[n, :, :, cols], sib_buf.at[n, :, :, cols], rs_send.at[n, 0], rs_recv.at[n, 0],
            device_id={"c": 1 - c}, device_id_type=MESH,
        )

    def to_y(n, kind, up):
        src, dst = (far_src, far_buf) if kind == 0 else (y_src, y_buf)
        cols = pl.ds(0, wide(n) // 2 if kind == 0 else wide(n))
        k = 0 if up else 1
        sem = 1 + 2 * kind + k
        return pltpu.make_async_remote_copy(
            src.at[n, k, :, cols], dst.at[n, k, :, cols], rs_send.at[n, sem], rs_recv.at[n, sem],
            device_id={"y": lax.rem(y + (1 if up else NY - 1), NY)}, device_id_type=MESH,
        )

    def place(i):
        return lax.rem(z + DZ[i] + NZ, NZ)

    def product(n):
        for k, i in enumerate(COLS[n]):
            full_part[n, :, k * slab : (k + 1) * slab] = dg(hid_ref[...], wd[place(i)].reshape(slab, hidden), 1, 1)
        for yy in range(NY):
            sib_src[n, yy, :, : wide(n)] = full_part[n, block_rows(yy * NC + 1 - c), : wide(n)].astype(BF16)
        go(to_mate(n))

    def chip_sum(n):
        to_mate(n).wait_recv()
        w, h = wide(n), wide(n) // 2

        def of(d):
            yy = lax.rem(y + d, NY)
            return full_part[n, block_rows(yy * NC + c), :w] + sib_buf[n, yy, :, :w].astype(F32)

        far = of(2).astype(BF16)
        far_src[n, 0, :, :h] = far[:, :h]
        far_src[n, 1, :, :h] = far[:, h:]
        go(to_y(n, 0, True))
        go(to_y(n, 0, False))
        own_part[n, :, :w] = of(0)
        pair[n, 0, :, :w] = of(1)
        pair[n, 1, :, :w] = of(3)

    def ring_sum(n):
        w, h = wide(n), wide(n) // 2
        to_y(n, 0, True).wait_recv()
        y_src[n, 0, :, :h] = (pair[n, 0, :, :h] + far_buf[n, 0, :, :h].astype(F32)).astype(BF16)
        y_src[n, 0, :, h:w] = pair[n, 0, :, h:w].astype(BF16)
        go(to_y(n, 1, True))
        to_y(n, 0, False).wait_recv()
        y_src[n, 1, :, :h] = pair[n, 1, :, :h].astype(BF16)
        y_src[n, 1, :, h:w] = (pair[n, 1, :, h:w] + far_buf[n, 1, :, :h].astype(F32)).astype(BF16)
        go(to_y(n, 1, False))

    def finish(n):
        for up in (True, False):
            to_y(n, 1, up).wait_recv()
        for k, i in enumerate(COLS[n]):
            at = slice(k * slab, (k + 1) * slab)
            acc = own_part[n, :, at] + y_buf[n, 0, :, at].astype(F32) + y_buf[n, 1, :, at].astype(F32)
            cols = pl.ds(pl.multiple_of(place(i) * slab, slab), slab)
            out_ref[:, cols] = (mid_ref[block_rows(tp), cols].astype(F32) + 0.5 * acc).astype(BF16)

    for n in range(len(COLS)):
        mark(f"d{n}")
        g.serve(f"d{n}")
        if n > 0:
            chip_sum(n - 1)
        if n > 1:
            ring_sum(n - 2)
        mark(f"w{n}")
        for i in COLS[n]:
            g.slab(DQ, DP, i)
        mark(f"p{n}")
        product(n)
    last = len(COLS) - 1
    mark("cs3")
    chip_sum(last)
    mark("rs2")
    ring_sum(last - 1)
    mark("fin01")
    for n in range(last - 1):
        finish(n)
    mark("rs3")
    ring_sum(last)
    mark("fin2")
    finish(last - 1)
    mark("fin3")
    finish(last)
    mark("sendwait")
    for copy in sends:
        copy.wait_send()
    for d in range(1, ZG):
        pl.when(place_z + d < ZG)(lambda d=d: z_state(d).wait_send())

    @pl.when(z == ZG - 1)
    def _():
        for d in range(1, ZG + 1):
            z_half(d).wait_send()

    mark(None)


def per_device(
    resid, queries, keys, values, decay_input_part, decay_channel_offset, decay_head_extra, correction_rate_input,
    correction_rate_offset, head_norm_gain, mixer_output_weight, feedforward_norm_gain, gate_weight, up_weight, down_weight,
):
    tokens = queries.shape[0]
    share, width = resid.shape
    shard, hidden = gate_weight.shape
    vm, sem = pltpu.VMEM, pltpu.SemaphoreType.DMA
    flat = pl.BlockSpec(memory_space=pltpu.VMEM)
    there = pl.BlockSpec(memory_space=pl.ANY)
    slab = width // NZ
    parts, wide = len(COLS), max(map(len, COLS)) * slab
    return pl.pallas_call(
        kernel,
        name="layer",
        out_shape=pltpu.VMEM((share, width), BF16),
        in_specs=[there] * 15,
        out_specs=flat,
        scratch_shapes=[
            *[vm((tokens, LANES), BF16)] * 5, *[vm((1, LANES), F32)] * 3, vm((LANES // HEAD, tokens), F32), vm((1, width), F32),
            vm((NZ, NX, shard, 2 * hidden), BF16), vm((NZ, NX, shard, hidden), BF16),
            vm((shard, hidden), BF16), vm((shard, hidden), BF16),
            vm(mixer_output_weight.shape, BF16), vm((tokens, width), BF16),
            vm((tokens, LANES), F32),
            vm((CHUNKS, LANES, LANES), F32), vm((CHUNKS, LANES, LANES), F32),
            vm((CHUNKS, LANES, LANES), F32), vm((CHUNKS, LANES, LANES), F32),
            vm((tokens, LANES), F32), vm((tokens, LANES), F32),
            vm((LANES, LANES), BF16), vm((NX - 1, LANES, LANES), BF16), vm((2 * LANES, LANES), F32),
            vm((LANES, LANES), BF16), vm((ZG - 1, LANES, LANES), BF16), vm((2 * LANES, LANES), F32),
            vm((HEAD, LANES), BF16), vm((HEAD, LANES), BF16),
            vm((tokens, NT * LANES), BF16), vm((tokens, width), BF16), vm((tokens, width), BF16), vm((tokens, hidden), BF16),
            vm((parts, tokens, wide), F32), vm((parts, share, wide), F32), vm((parts, 2, share, wide), F32),
            vm((parts, NY, share, wide), BF16), vm((parts, NY, share, wide), BF16),
            vm((parts, 2, share, wide // 2), BF16), vm((parts, 2, share, wide // 2), BF16),
            vm((parts, 2, share, wide), BF16), vm((parts, 2, share, wide), BF16),
            sem((15,)), sem((10, 8)), sem((10, 8)), sem((18, 4)), sem((18, 4)),
            sem((NX + 2 * ZG - 2,)), sem((NX + ZG - 1,)), sem((10,)), sem((10,)), sem((10,)), sem((10,)),
            sem((parts, 5)), sem((parts, 5)),
        ],
        compiler_params=pltpu.CompilerParams(collective_id=0, has_side_effects=True),
    )(
        queries, keys, values, decay_input_part, correction_rate_input,
        decay_channel_offset[None], correction_rate_offset[None], head_norm_gain[None], decay_head_extra.T,
        feedforward_norm_gain[None], resid, mixer_output_weight, gate_weight, up_weight, down_weight.T,
    )


def solution(mesh):
    torus = Mesh(mesh.devices.reshape(NZ, NX, NY, NC), SP_TP)
    in_specs = (
        P(SP_TP, None), P(SP, TP), P(SP, TP), P(SP, TP), P(SP, TP), P(TP), P(SP, TP), P(SP, TP), P(TP), P(TP),
        P(), P(), P(SP, TP), P(SP, TP), P(TP, SP),
    )
    return jax.shard_map(per_device, mesh=torus, in_specs=in_specs, out_specs=P(SP_TP, None), check_vma=False)
```

```python
import functools

import jax
import jax.numpy as jnp
from jax import lax
from jax.experimental import pallas as pl
from jax.experimental.pallas import tpu as pltpu
from jax.sharding import Mesh
from jax.sharding import PartitionSpec as P

F32, BF16 = jnp.float32, jnp.bfloat16
MESH = pl.DeviceIdType.MESH
HEAD, LANES, CH = 64, 128, 64
NZ, NX, NY, NC = 8, 4, 4, 2
NT = NY * NC
ZG = NZ // 2
CHUNKS = 6
GROUP = 3
COLS = ((0, 1, 2), (3, 4), (5, 6), (7,))
SP, TP, SP_TP = ("z", "x"), ("y", "c"), ("z", "x", "y", "c")


def dg(a, b, ca=1, cb=0):
    return lax.dot_general(a, b, (((ca,), (cb,)), ((), ())), preferred_element_type=F32)


def halves(x):
    hi = x.astype(BF16)
    return hi, (x - hi.astype(F32)).astype(BF16)


def mm(a, b, ca=1, cb=0):
    return dg(a[0], b[0], ca, cb) + dg(a[0], b[1], ca, cb) + dg(a[1], b[0], ca, cb)


def thirds(x):
    hi = x.astype(BF16)
    rest = x - hi.astype(F32)
    mid = rest.astype(BF16)
    return hi, mid, (rest - mid.astype(F32)).astype(BF16)


def iota(shape, dim):
    return lax.broadcasted_iota(jnp.int32, shape, dim)


def first_head(rows):
    return iota((rows, LANES), 1) < HEAD


def stacked(x):
    own = first_head(x.shape[0])
    zero = jnp.zeros_like(x)
    return jnp.concatenate([jnp.where(own, x, zero), jnp.where(own, zero, x)], axis=0)


def folded(x):
    half = x.shape[0] // 2
    return x[:half] + x[half:]


def head_ones():
    return (iota((LANES, LANES), 0) // HEAD == iota((LANES, LANES), 1) // HEAD).astype(BF16)


def head_sum(x, ones):
    hi, lo = halves(x)
    return dg(hi, ones) + dg(lo, ones)


def sigmoid(x):
    return 1.0 / (1.0 + jnp.exp(-x))


def mixer_group(first, serve, q_ref, k_ref, v_ref, dip_ref, cri_ref, dco_ref, cro_ref, extra_ref, m_ref, n_ref, r_ref, o_ref):
    ids = range(first, first + GROUP)
    ones = head_ones()
    row, col = iota((LANES, LANES), 0), iota((LANES, LANES), 1)
    eye = (row == col).astype(F32)
    low = (iota((CH, CH), 0) >= iota((CH, CH), 1)).astype(BF16)
    ends, us, bts, avs, reads, vs = [], [], [], [], [], []
    invs, offs, qks = [], [], []
    for c in ids:
        rows = pl.ds(c * CH, CH)
        q, k, v = (r[rows, :].astype(F32) for r in (q_ref, k_ref, v_ref))
        pre = dco_ref[...] + dip_ref[rows, :].astype(F32)
        log_decay = -(sigmoid(pre) * 0.6065306597126334) - extra_ref[rows, :]
        unit = k * lax.rsqrt(head_sum(k * k, ones) + 1e-6)
        b = unit * sigmoid(cro_ref[...] + cri_ref[rows, :].astype(F32))
        total = sum(dg(low, part) for part in thirds(log_decay))
        before = total - log_decay
        mid, end = total[CH // 2 - 1 : CH // 2], total[CH - 1 :]
        up, down = jnp.exp(total - mid), jnp.exp(mid - total)
        up_before = jnp.exp(before - mid)
        rest = jnp.exp(end - total)
        left = halves(jnp.concatenate([stacked(unit * up_before), stacked(q * up)], axis=0))
        right = halves(jnp.concatenate([stacked(k * down), stacked(b * down)], axis=0))
        a = mm(left, right, 1, 1)
        a_uk = jnp.where(row > col, a[:LANES, :LANES], 0.0)
        a_qk = jnp.where(row >= col, a[LANES:, :LANES], 0.0)
        a_qb = jnp.where(row >= col, a[LANES:, LANES:], 0.0)
        offs.append(a[:LANES, LANES:])
        vst = halves(stacked(v))
        av = mm(halves(jnp.concatenate([a_uk, a_qk], axis=0)), vst)
        us.append(halves(jnp.concatenate([stacked(unit * jnp.exp(before)), av[:LANES]], axis=1)))
        avs.append(av[LANES:])
        qks.append(halves(a_qb))
        reads.append(stacked(q * jnp.exp(total)))
        bts.append(halves(stacked(b * rest)))
        ends.append((jnp.exp(end), mm(vst, halves(stacked(k * rest)), 0, 0)))
    serve(first)
    size = 1
    while size < CH:
        inside = (row // (2 * size) == col // (2 * size)) & (row // size != col // size) & (row > col)
        for i in range(GROUP):
            part = jnp.where(inside, offs[i], 0.0)
            if size == 1:
                invs.append(eye - part)
            else:
                inv = halves(invs[i])
                invs[i] = invs[i] - mm(halves(mm(inv, halves(part))), inv)
        size *= 2
    serve(first + 1)
    for i, c in enumerate(ids):
        wu = mm(halves(invs[i]), us[i])
        wu2 = halves(wu)
        ro = mm(qks[i], wu2)
        r_ref[c] = reads[i] - ro[:, :LANES]
        o_ref[c] = avs[i] - ro[:, LANES:]
        mn = mm(wu2, bts[i], 0, 0)
        decay, kv = ends[i]
        m_ref[c] = jnp.where(row == col, decay, 0.0) - mn[:LANES]
        n_ref[c] = kv - mn[LANES:]


def unpacked(message):
    wide = message.astype(F32)
    return stacked(wide[:HEAD]).astype(BF16), stacked(wide[HEAD:])


def packed(trans, state):
    return jnp.concatenate([folded(trans), folded(state)], axis=0).astype(BF16)


def after(total, message):
    trans, state = unpacked(message)
    hi, lo = halves(total)
    out = dg(hi, trans) + dg(lo, trans)
    return jnp.concatenate([out[:LANES], out[LANES:] + state], axis=0)


GQ, GP, DQ, DP = 0, 1, 2, 3
PARTS = ((0, 24, 40, True), (0, 0, 24, False), (1, 16, 16, True), (1, 0, 16, False))
Z_RINGS = (0, 2, 1, 6)
X_RINGS = (0, 16, 8, 17)
DZ = (0, -1, 1, -2, 2, -3, 3, 4)
DX = (0, 1, -1, 2)
Z_ON, Z_FIRST, X_FIRST, X_ON = 0, 1, 2, 3
SCHEDULE = {
    "start": (
        (2, 0, 0, 0), (2, 1, 0, 0), (1, 1, 0, 0), (1, 0, 0, 0),
    ),
    "a0": (
        (2, 3, 0, 0), (1, 3, 0, 0),
    ),
    "a1": (
        (2, 2, 0, 0), (1, 2, 0, 0),
    ),
    "a2": (
        (0, 1, 0, 1),
    ),
    "a3": (
        (2, 0, 1, 0), (3, 1, 0, 0), (0, 0, 0, 1), (1, 1, 1, 0), (1, 1, 2, 0),
    ),
    "a4": (
        (3, 3, 0, 0),
    ),
    "xsent": (
        (2, 0, 2, 0), (3, 0, 0, 0), (0, 1, 0, 2), (3, 0, 1, 0), (2, 0, 3, 0), (2, 0, 4, 0),
        (0, 0, 0, 2),
    ),
    "zsent": (
        (0, 1, 1, 1), (0, 1, 2, 1), (1, 1, 3, 0), (0, 1, 0, 3), (3, 0, 2, 0), (2, 0, 5, 0),
        (2, 0, 6, 0), (0, 0, 0, 3),
    ),
    "z2sent": (
        (3, 0, 3, 0), (0, 1, 1, 2), (0, 1, 2, 2), (3, 0, 4, 0), (0, 1, 3, 1), (2, 0, 7, 0),
        (0, 2, 0, 1), (3, 0, 5, 0), (1, 3, 1, 0),
    ),
    "ag1": (
        (0, 1, 1, 3), (3, 0, 6, 0), (1, 3, 2, 0), (0, 1, 2, 3), (0, 1, 3, 2),
    ),
    "ag2": (
        (3, 2, 0, 0), (1, 3, 3, 0), (2, 2, 1, 0), (0, 2, 0, 2), (2, 2, 2, 0), (3, 0, 7, 0),
        (0, 3, 0, 1),
    ),
    "ag3": (
        (0, 3, 1, 1), (2, 2, 3, 0),
    ),
    "pr0": (
        (0, 1, 3, 3),
    ),
    "pr1": (
        (2, 2, 4, 0), (0, 3, 2, 1),
    ),
    "pr2": (
        (3, 2, 1, 0), (0, 3, 3, 1),
    ),
    "pr3": (
        (3, 2, 2, 0), (2, 2, 5, 0), (0, 2, 0, 3),
    ),
    "gu": (
        (0, 3, 0, 2), (2, 2, 6, 0), (0, 3, 1, 2), (3, 2, 3, 0),
    ),
    "d0": (
        (3, 2, 4, 0), (2, 2, 7, 0), (0, 3, 2, 2), (0, 3, 3, 2),
    ),
    "d1": (
        (3, 2, 5, 0), (0, 3, 0, 3), (3, 2, 6, 0), (0, 3, 1, 3),
    ),
    "d2": (
        (0, 3, 2, 3), (3, 2, 7, 0), (0, 3, 3, 3),
    ),
}


class Gather:
    def __init__(self, bufs, send_z, recv_z, send_x, recv_x, sends):
        self.bufs, self.sends, self.here, self.done = bufs, sends, set(), set()
        self.sems = {"z": (send_z, recv_z), "x": (send_x, recv_x)}
        self.place = {"z": lax.axis_index("z"), "x": lax.axis_index("x")}

    def copy(self, axis, part, i, hop, right, got):
        buf, first, rows, z_first = PARTS[part]
        sign, far = (1 if right else -1), {"z": 4, "x": 2}[axis]
        size = {"z": NZ, "x": NX}
        back = -sign * (hop if got else hop - 1)
        dz, dx = (back, DX[i]) if axis == "z" else (DZ[i], back)
        ref = self.bufs[buf].at[lax.rem(self.place["z"] + dz + NZ, NZ), lax.rem(self.place["x"] + dx + NX, NX)]
        if hop == far:
            cut = (rows // 8 + i % 2) // 2 * 8
            first, rows = (first, cut) if right else (first + cut, rows - cut)
        ref = ref.at[pl.ds(first, rows)]
        ring = (Z_RINGS if axis == "z" else X_RINGS)[part] + i
        slot = hop - 1 + (0 if right else far)
        send, recv = self.sems[axis]
        return pltpu.make_async_remote_copy(
            ref, ref, send.at[ring, slot], recv.at[ring, slot],
            device_id={axis: lax.rem(self.place[axis] + sign + size[axis], size[axis])}, device_id_type=MESH,
        )

    def send(self, axis, part, i, hop):
        for right in (True, False):
            copy = self.copy(axis, part, i, hop, right, False)
            copy.start()
            self.sends.append(copy)

    def need(self, axis, part, i, hop):
        if (axis, part, i, hop) not in self.here:
            self.here.add((axis, part, i, hop))
            for right in (True, False):
                self.copy(axis, part, i, hop, right, True).wait_recv()

    def do(self, kind, part, i, hop):
        self.done.add((kind, part, i, hop))
        z_first = PARTS[part][3]
        if kind == Z_ON:
            self.need("z", part, i, hop)
            self.send("z", part, i, hop + 1)
        elif kind == Z_FIRST:
            if not z_first and i:
                self.need("x", part, 0, 1 if i < 3 else 2)
            self.send("z", part, i, 1)
        elif kind == X_FIRST:
            if z_first and i:
                self.need("z", part, 0, (i + 1) // 2)
            self.send("x", part, i, 1)
        else:
            self.need("x", part, i, 1)
            self.send("x", part, i, 2)

    def serve(self, point):
        for task in SCHEDULE.get(point, ()):
            self.do(*task)

    def whole(self, part):
        for i in range(8 if PARTS[part][3] else 1):
            self.need("x", part, i, 1)
            self.need("x", part, i, 2)
        for i in range(1 if PARTS[part][3] else 4):
            for hop in range(1, 5):
                self.need("z", part, i, hop)

    def slab(self, q, p, i):
        hop = (i + 1) // 2
        if i:
            self.need("z", q, 0, hop)
            for j in range(4):
                self.need("z", p, j, hop)
        for part, ring in ((q, i), (p, 0)):
            self.need("x", part, ring, 1)
            self.need("x", part, ring, 2)


class Spread:
    def __init__(self, block, send_sem, recv_sem, sends):
        self.block, self.send_sem, self.recv_sem, self.sends = block, send_sem, recv_sem, sends
        self.y, self.c = lax.axis_index("y"), lax.axis_index("c")

    def along_y(self, sem, dy, up, half):
        ref = self.block(lax.rem(self.y + dy + NY, NY) * NC + self.c, half)
        return pltpu.make_async_remote_copy(
            ref, ref, self.send_sem.at[sem], self.recv_sem.at[sem],
            device_id={"y": lax.rem(self.y + (1 if up else NY - 1), NY)}, device_id_type=MESH,
        )

    def across(self, sem, dy, mine):
        ref = self.block(lax.rem(self.y + dy + NY, NY) * NC + (self.c if mine else 1 - self.c), None)
        return pltpu.make_async_remote_copy(
            ref, ref, self.send_sem.at[sem], self.recv_sem.at[sem], device_id={"c": 1 - self.c}, device_id_type=MESH
        )

    def go(self, copy):
        copy.start()
        self.sends.append(copy)

    def start(self):
        for half in (0, 1):
            self.go(self.along_y(half, 0, True, half))
            self.go(self.along_y(2 + half, 0, False, 1 - half))
        self.go(self.across(6, 0, True))

    def relay(self):
        self.along_y(0, -1, True, 0).wait_recv()
        self.go(self.along_y(4, -1, True, 0))
        self.along_y(2, 1, False, 1).wait_recv()
        self.go(self.along_y(5, 1, False, 1))

    def near(self):
        self.along_y(1, -1, True, 1).wait_recv()
        self.go(self.across(7, -1, True))
        self.along_y(3, 1, False, 0).wait_recv()
        self.go(self.across(8, 1, True))

    def far(self):
        self.along_y(4, 2, True, 0).wait_recv()
        self.along_y(5, 2, False, 1).wait_recv()
        self.go(self.across(9, 2, True))

    def finish(self):
        for sem, dy in ((6, 0), (7, -1), (8, 1), (9, 2)):
            self.across(sem, dy, False).wait_recv()


_open = []


def mark(name):
    if _open:
        _open.pop().__exit__(None, None, None)
    if name:
        _open.append(jax.named_scope(name))
        _open[-1].__enter__()


def kernel(
    q_hbm, k_hbm, v_hbm, dip_hbm, cri_hbm, dco_hbm, cro_hbm, gain_hbm, extra_t_hbm, fng_hbm,
    resid_hbm, wo_hbm, gate_hbm, up_hbm, down_hbm,
    out_ref,
    q_ref, k_ref, v_ref, dip_ref, cri_ref, dco_ref, cro_ref, gain_ref, extra_t_ref, fng_ref,
    wgu, wd, g_in, u_in, d_in, wo, resid,
    extra_ref, m_ref, n_ref, r_ref, o_ref, gm_ref, hm_ref,
    tot_ref, xbuf, xpre, zsrc, zbuf, s_ref, z2src, z2buf,
    mix_all, mid_ref, rows, hid_ref,
    full_part, own_part, pair, sib_src, sib_buf, far_src, far_buf, y_src, y_buf, far_out, far_in,
    local_sem, send_z, recv_z, send_x, recv_x,
    st_send, st_recv, res_send, res_recv, ag_send, ag_recv, rs_send, rs_recv,
):
    z, x, y, c = (lax.axis_index(n) for n in SP_TP)
    tp = y * NC + c
    sends = []
    tokens, width = rows.shape
    share = tokens // NT

    def block_rows(i):
        return pl.ds(pl.multiple_of(i * share, 16), share)

    def go(copy):
        copy.start()
        sends.append(copy)

    mark("barrier")
    own = [
        pltpu.make_async_copy(src, dst, local_sem.at[i])
        for i, (src, dst) in enumerate(
            ((gate_hbm, g_in), (up_hbm, u_in), (down_hbm, d_in), (resid_hbm, resid.at[block_rows(tp)]),
             (extra_t_hbm, extra_t_ref), (k_hbm, k_ref), (q_hbm, q_ref), (v_hbm, v_ref), (dip_hbm, dip_ref),
             (cri_hbm, cri_ref), (dco_hbm, dco_ref), (cro_hbm, cro_ref), (gain_hbm, gain_ref), (fng_hbm, fng_ref), (wo_hbm, wo))
        )
    ]
    barrier = pltpu.get_barrier_semaphore()
    peers = [{"x": lax.rem(x + d, NX)} for d in range(1, NX)]
    peers += [{"z": lax.rem(z + d, NZ)} for d in range(1, NZ)]
    peers += [{"y": lax.rem(y + d, NY)} for d in range(1, NY)] + [{"c": 1 - c}]
    for peer in peers:
        pl.semaphore_signal(barrier, inc=1, device_id=peer, device_id_type=MESH)
    for copy in own:
        copy.start()
    for copy in own[:2]:
        copy.wait()
    hidden = g_in.shape[1]
    full = hidden // LANES * LANES

    def side_by_side(left, right):
        tail = jnp.concatenate([left[:, full:].astype(F32), right[:, full:].astype(F32)], axis=1)
        return jnp.concatenate([left[:, :full], right[:, :full], tail.astype(BF16)], axis=1)

    wgu[z, x] = side_by_side(g_in[...], u_in[...])
    own[2].wait()
    wd[z, x] = side_by_side(d_in[: d_in.shape[0] // 2], d_in[d_in.shape[0] // 2 :])
    own[4].wait()
    extra_t = jnp.concatenate([extra_t_ref[...], jnp.zeros((6, extra_t_ref.shape[1]), F32)], axis=0)
    pick = (iota((8, LANES), 0) == iota((8, LANES), 1) // HEAD).astype(BF16)
    extra_ref[...] = sum(dg(part, pick, 0, 0) for part in thirds(extra_t))
    pl.semaphore_wait(barrier, len(peers))

    g = Gather((wgu, wd), send_z, recv_z, send_x, recv_x, sends)
    g.serve("start")

    def resid_block(i, half):
        cols = pl.ds(0, width) if half is None else pl.ds(half * (width // 2), width // 2)
        return resid.at[block_rows(i), cols]

    def mix_block(i, half):
        part = pl.ds(0, tokens) if half is None else pl.ds(half * (tokens // 2), tokens // 2)
        return mix_all.at[part, pl.ds(pl.multiple_of(i * LANES, LANES), LANES)]

    own[3].wait()
    res = Spread(resid_block, res_send, res_recv, sends)
    res.start()

    mix = functools.partial(
        mixer_group, serve=lambda i: g.serve(f"a{i}"), q_ref=q_ref, k_ref=k_ref, v_ref=v_ref, dip_ref=dip_ref, cri_ref=cri_ref, dco_ref=dco_ref,
        cro_ref=cro_ref, extra_ref=extra_ref, m_ref=m_ref, n_ref=n_ref, r_ref=r_ref, o_ref=o_ref,
    )
    for copy in own[5:14]:
        copy.wait()
    mark("mix0")
    mix(0)
    mark("s1")
    g.serve("a2")
    res.relay()
    mark("mix1")
    mix(GROUP)
    mark("s2")
    g.serve("a5")
    res.near()
    res.far()
    mark("prefix")

    row, col = iota((LANES, LANES), 0), iota((LANES, LANES), 1)
    start = jnp.concatenate([(row == col).astype(F32), jnp.zeros((LANES, LANES), F32)], axis=0)
    total = start
    for i in range(CHUNKS):
        split = halves(total)
        step = mm(split, halves(m_ref[i]))
        gh = mm(halves(r_ref[i]), split, 1, 1)
        rows_i = pl.ds(i * CH, CH)
        gm_ref[rows_i, :] = folded(gh[:, :LANES])
        hm_ref[rows_i, :] = folded(gh[:, LANES:] + o_ref[i])
        total = jnp.concatenate([step[:LANES], step[LANES:] + n_ref[i]], axis=0)
    tot_ref[...] = packed(total[:LANES], total[LANES:])

    def x_state(d):
        return pltpu.make_async_remote_copy(
            tot_ref, xbuf.at[d - 1], st_send.at[d - 1], st_recv.at[d - 1],
            device_id={"x": lax.rem(x + d, NX)}, device_id_type=MESH,
        )

    for d in range(1, NX):
        go(x_state(d))
    mark("s2")
    g.serve("xsent")
    mark("xstate")
    for d in range(1, NX):
        x_state(d).wait_recv()
    mark("xcomb")
    total = start
    prefix = total
    for i in range(NX):
        prefix = jnp.where(x == i, total, prefix)
        message = tot_ref[...]
        for d in range(1, NX):
            message = jnp.where(lax.rem(x - i + NX, NX) == d, xbuf[d - 1], message)
        total = after(total, message)
    xpre[...] = prefix
    zsrc[...] = packed(total[:LANES], total[LANES:])

    place_z, far_half = lax.rem(z, ZG), z >= ZG

    def z_state(d):
        return pltpu.make_async_remote_copy(
            zsrc, zbuf.at[d - 1], st_send.at[NX - 2 + d], st_recv.at[NX - 2 + d],
            device_id={"z": lax.rem(z + d, NZ)}, device_id_type=MESH,
        )

    def z_half(d):
        return pltpu.make_async_remote_copy(
            z2src, z2buf, st_send.at[NX + ZG - 3 + d], st_recv.at[NX + ZG - 2],
            device_id={"z": lax.rem(z + d, NZ)}, device_id_type=MESH,
        )

    for d in range(1, ZG):
        pl.when(place_z + d < ZG)(lambda d=d: z_state(d).start())
    mark("s3")
    g.serve("zsent")
    mark("zstate")
    s_ref[...] = start
    for d in range(ZG - 1, 0, -1):

        @pl.when(place_z >= d)
        def _(d=d):
            z_state(d).wait_recv()
            s_ref[...] = after(s_ref[...], zbuf[d - 1])

    @pl.when(z == ZG - 1)
    def _():
        z2src[...] = folded(after(s_ref[...], zsrc[...])[LANES:]).astype(BF16)
        for d in range(1, ZG + 1):
            z_half(d).start()

    mark("s3b")
    g.serve("z2sent")
    mark("zhalf")

    @pl.when(far_half)
    def _():
        z_half(1).wait_recv()
        s_ref[LANES:] += mm(halves(stacked(z2buf[...].astype(F32))), halves(s_ref[:LANES]))

    mark("read")
    incoming = mm(halves(s_ref[LANES:]), halves(xpre[:LANES])) + xpre[LANES:]
    read = mm(halves(gm_ref[...]), halves(incoming), 1, 1) + hm_ref[...]
    ones = head_ones()
    center = read - head_sum(read, ones) * (1.0 / HEAD)
    spread = head_sum(center * center, ones) * (1.0 / HEAD)
    mine = pl.ds(pl.multiple_of(tp * LANES, LANES), LANES)
    mix_all[:, mine] = (center * lax.rsqrt(spread + 1e-5) * gain_ref[...]).astype(BF16)
    mixed = Spread(mix_block, ag_send, ag_recv, sends)
    mixed.start()
    mark("ag1")
    g.serve("ag1")
    mark("ag1w")
    mixed.relay()
    mark("ag2")
    g.serve("ag2")
    mark("ag2w")
    mixed.near()
    mixed.far()
    mark("ag3")
    g.serve("ag3")
    mark("ag3w")
    own[14].wait()
    res.finish()
    mixed.finish()

    tile = 512
    square = jnp.zeros((tokens, 1), F32)
    for i in range(width // tile):
        mark(f"pr{i}")
        cols = pl.ds(i * tile, tile)
        proj = jnp.dot(mix_all[...], wo[:, cols], preferred_element_type=F32)
        mid = (resid[:, cols].astype(F32) + proj).astype(BF16)
        mid_ref[:, cols] = mid
        mid = mid.astype(F32)
        square += jnp.sum(mid * mid, axis=-1, keepdims=True)
        mark(f"sp{i}")
        g.serve(f"pr{i}")
    mark("norm")
    scale = lax.rsqrt(square * (1.0 / width) + 1e-6)
    for i in range(width // tile):
        cols = pl.ds(i * tile, tile)
        rows[:, cols] = (mid_ref[:, cols].astype(F32) * scale * fng_ref[:, cols]).astype(BF16)
    early = len(sends)
    mark("gu")
    g.serve("gu")
    g.whole(GQ)
    g.whole(GP)

    mark("gateup")
    both = jnp.dot(rows[...], wgu[...].reshape(width, 2 * hidden), preferred_element_type=F32)

    def gated(gate, upper):
        return (gate * sigmoid(gate) * upper).astype(BF16)

    rest = hidden - full
    hid_ref[:, :full] = gated(both[:, :full], both[:, full : 2 * full])
    tail = gated(both[:, 2 * full : 2 * full + rest], both[:, 2 * full + rest :]).astype(F32)
    none = jnp.zeros((tokens, LANES - rest), F32)
    hid_ref[:, full : full + LANES] = jnp.concatenate([tail, none], axis=1).astype(BF16)
    hid_ref[:, full + LANES :] = jnp.concatenate([none, tail], axis=1).astype(BF16)

    slab = width // NZ

    def wide(n):
        return len(COLS[n]) * slab

    def to_mate(n):
        cols = pl.ds(0, wide(n))
        return pltpu.make_async_remote_copy(
            sib_src.at[n, :, :, cols], sib_buf.at[n, :, :, cols], rs_send.at[n, 0], rs_recv.at[n, 0],
            device_id={"c": 1 - c}, device_id_type=MESH,
        )

    def to_y(n, kind, up):
        src, dst = (far_src, far_buf) if kind == 0 else (y_src, y_buf)
        cols = pl.ds(0, wide(n) // 2 if kind == 0 else wide(n))
        k = 0 if up else 1
        sem = 1 + 2 * kind + k
        return pltpu.make_async_remote_copy(
            src.at[n, k, :, cols], dst.at[n, k, :, cols], rs_send.at[n, sem], rs_recv.at[n, sem],
            device_id={"y": lax.rem(y + (1 if up else NY - 1), NY)}, device_id_type=MESH,
        )

    def straight():
        return pltpu.make_async_remote_copy(
            far_out, far_in, rs_send.at[last, 1], rs_recv.at[last, 1],
            device_id={"y": lax.rem(y + 2, NY)}, device_id_type=MESH,
        )

    def place(i):
        return lax.rem(z + DZ[i] + NZ, NZ)

    def product(n):
        for k, i in enumerate(COLS[n]):
            weights = wd[place(i)].reshape(slab // 2, 2 * hidden)
            for side in range(2):
                left = jnp.concatenate([hid_ref[:, :full], hid_ref[:, full + side * LANES : full + (side + 1) * LANES]], axis=1)
                right = jnp.concatenate([weights[:, side * full : (side + 1) * full], weights[:, 2 * full :]], axis=1)
                at = k * slab + side * (slab // 2)
                full_part[n, :, at : at + slab // 2] = dg(left, right, 1, 1)
        for yy in range(NY):
            sib_src[n, yy, :, : wide(n)] = full_part[n, block_rows(yy * NC + 1 - c), : wide(n)].astype(BF16)
        go(to_mate(n))

    def chip_sum(n):
        to_mate(n).wait_recv()
        w, h = wide(n), wide(n) // 2

        def of(d):
            yy = lax.rem(y + d, NY)
            return full_part[n, block_rows(yy * NC + c), :w] + sib_buf[n, yy, :, :w].astype(F32)

        if n == last:
            far_out[...] = of(2).astype(BF16)
            go(straight())
            y_src[n, 0, :, :w] = of(1).astype(BF16)
            go(to_y(n, 1, True))
            y_src[n, 1, :, :w] = of(3).astype(BF16)
            go(to_y(n, 1, False))
            own_part[n, :, :w] = of(0)
            return
        far = of(2).astype(BF16)
        far_src[n, 0, :, :h] = far[:, :h]
        far_src[n, 1, :, :h] = far[:, h:]
        go(to_y(n, 0, True))
        go(to_y(n, 0, False))
        own_part[n, :, :w] = of(0)
        pair[n, 0, :, :w] = of(1)
        pair[n, 1, :, :w] = of(3)

    def ring_sum(n):
        w, h = wide(n), wide(n) // 2
        to_y(n, 0, True).wait_recv()
        y_src[n, 0, :, :h] = (pair[n, 0, :, :h] + far_buf[n, 0, :, :h].astype(F32)).astype(BF16)
        y_src[n, 0, :, h:w] = pair[n, 0, :, h:w].astype(BF16)
        go(to_y(n, 1, True))
        to_y(n, 0, False).wait_recv()
        y_src[n, 1, :, :h] = pair[n, 1, :, :h].astype(BF16)
        y_src[n, 1, :, h:w] = (pair[n, 1, :, h:w] + far_buf[n, 1, :, :h].astype(F32)).astype(BF16)
        go(to_y(n, 1, False))

    def in_order(packed_cols):
        block = slab // NX // 2
        group = iota((share, LANES), 1) // block
        tiles = []
        for t in range(slab // LANES):
            out = None
            for to in range(LANES // block):
                at = LANES // block // 2 * t + to // 2
                shifted = packed_cols[:, (to % 2) * (slab // 2) : (to % 2 + 1) * (slab // 2)]
                shift = (to - at) * block % LANES
                shifted = pltpu.roll(shifted, shift, 1) if shift else shifted
                out = shifted if out is None else jnp.where(group == to, shifted, out)
            tiles.append(out)
        return jnp.concatenate(tiles, axis=1)

    last = len(COLS) - 1

    def finish(n):
        for up in (True, False):
            to_y(n, 1, up).wait_recv()
        if n == last:
            straight().wait_recv()
        for k, i in enumerate(COLS[n]):
            at = slice(k * slab, (k + 1) * slab)
            acc = own_part[n, :, at] + y_buf[n, 0, :, at].astype(F32) + y_buf[n, 1, :, at].astype(F32)
            if n == last:
                acc += far_in[...].astype(F32)
            acc = in_order(acc)
            cols = pl.ds(pl.multiple_of(place(i) * slab, slab), slab)
            out_ref[:, cols] = (mid_ref[block_rows(tp), cols].astype(F32) + 0.5 * acc).astype(BF16)

    for n in range(len(COLS)):
        mark(f"d{n}")
        g.serve(f"d{n}")
        if n > 0:
            chip_sum(n - 1)
        if n > 1:
            ring_sum(n - 2)
        if n == last:
            for copy in sends[:early]:
                copy.wait_send()
        mark(f"w{n}")
        for i in COLS[n]:
            g.slab(DQ, DP, i)
        mark(f"p{n}")
        product(n)
    mark("rs2")
    ring_sum(last - 1)
    mark("cs3")
    chip_sum(last)
    mark("fin0")
    for n in range(last - 1):
        finish(n)
    mark("fin2")
    finish(last - 1)
    mark("fin3")
    finish(last)
    mark("sendwait")
    for copy in sends[early:]:
        copy.wait_send()
    for d in range(1, ZG):
        pl.when(place_z + d < ZG)(lambda d=d: z_state(d).wait_send())

    @pl.when(z == ZG - 1)
    def _():
        for d in range(1, ZG + 1):
            z_half(d).wait_send()

    mark(None)


def per_device(
    resid, queries, keys, values, decay_input_part, decay_channel_offset, decay_head_extra, correction_rate_input,
    correction_rate_offset, head_norm_gain, mixer_output_weight, feedforward_norm_gain, gate_weight, up_weight, down_weight,
):
    tokens = queries.shape[0]
    share, width = resid.shape
    shard, hidden = gate_weight.shape
    vm, sem = pltpu.VMEM, pltpu.SemaphoreType.DMA
    flat = pl.BlockSpec(memory_space=pltpu.VMEM)
    there = pl.BlockSpec(memory_space=pl.ANY)
    slab = width // NZ
    parts, wide = len(COLS), max(map(len, COLS)) * slab
    return pl.pallas_call(
        kernel,
        name="layer",
        out_shape=pltpu.VMEM((share, width), BF16),
        in_specs=[there] * 15,
        out_specs=flat,
        scratch_shapes=[
            *[vm((tokens, LANES), BF16)] * 5, *[vm((1, LANES), F32)] * 3, vm((LANES // HEAD, tokens), F32), vm((1, width), F32),
            vm((NZ, NX, shard, 2 * hidden), BF16), vm((NZ, NX, shard // 2, 2 * hidden), BF16),
            vm((shard, hidden), BF16), vm((shard, hidden), BF16), vm((shard, hidden), BF16),
            vm(mixer_output_weight.shape, BF16), vm((tokens, width), BF16),
            vm((tokens, LANES), F32),
            vm((CHUNKS, LANES, LANES), F32), vm((CHUNKS, LANES, LANES), F32),
            vm((CHUNKS, LANES, LANES), F32), vm((CHUNKS, LANES, LANES), F32),
            vm((tokens, LANES), F32), vm((tokens, LANES), F32),
            vm((LANES, LANES), BF16), vm((NX - 1, LANES, LANES), BF16), vm((2 * LANES, LANES), F32),
            vm((LANES, LANES), BF16), vm((ZG - 1, LANES, LANES), BF16), vm((2 * LANES, LANES), F32),
            vm((HEAD, LANES), BF16), vm((HEAD, LANES), BF16),
            vm((tokens, NT * LANES), BF16), vm((tokens, width), BF16), vm((tokens, width), BF16), vm((tokens, hidden // LANES * LANES + 2 * LANES), BF16),
            vm((parts, tokens, wide), F32), vm((parts, share, wide), F32), vm((parts, 2, share, wide), F32),
            vm((parts, NY, share, wide), BF16), vm((parts, NY, share, wide), BF16),
            vm((parts, 2, share, wide // 2), BF16), vm((parts, 2, share, wide // 2), BF16),
            vm((parts, 2, share, wide), BF16), vm((parts, 2, share, wide), BF16),
            vm((share, len(COLS[-1]) * slab), BF16), vm((share, len(COLS[-1]) * slab), BF16),
            sem((15,)), sem((10, 8)), sem((10, 8)), sem((18, 4)), sem((18, 4)),
            sem((NX + 2 * ZG - 2,)), sem((NX + ZG - 1,)), sem((10,)), sem((10,)), sem((10,)), sem((10,)),
            sem((parts, 5)), sem((parts, 5)),
        ],
        compiler_params=pltpu.CompilerParams(collective_id=0, has_side_effects=True),
    )(
        queries, keys, values, decay_input_part, correction_rate_input,
        decay_channel_offset[None], correction_rate_offset[None], head_norm_gain[None], decay_head_extra.T,
        feedforward_norm_gain[None], resid, mixer_output_weight, gate_weight, up_weight, down_weight.T,
    )


def solution(mesh):
    torus = Mesh(mesh.devices.reshape(NZ, NX, NY, NC), SP_TP)
    in_specs = (
        P(SP_TP, None), P(SP, TP), P(SP, TP), P(SP, TP), P(SP, TP), P(TP), P(SP, TP), P(SP, TP), P(TP), P(TP),
        P(), P(), P(SP, TP), P(SP, TP), P(TP, SP),
    )
    return jax.shard_map(per_device, mesh=torus, in_specs=in_specs, out_specs=P(SP_TP, None), check_vma=False)
```

```python
import functools

import jax
import jax.numpy as jnp
from jax import lax
from jax.experimental import pallas as pl
from jax.experimental.pallas import tpu as pltpu
from jax.sharding import Mesh
from jax.sharding import PartitionSpec as P

F32, BF16 = jnp.float32, jnp.bfloat16
MESH = pl.DeviceIdType.MESH
HEAD, LANES, CH = 64, 128, 64
NZ, NX, NY, NC = 8, 4, 4, 2
NT = NY * NC
ZG = NZ // 2
CHUNKS = 6
GROUP = 3
COLS = ((0, 1, 2), (3, 4, 5), (6,), (7,))
SP, TP, SP_TP = ("z", "x"), ("y", "c"), ("z", "x", "y", "c")


def dg(a, b, ca=1, cb=0):
    return lax.dot_general(a, b, (((ca,), (cb,)), ((), ())), preferred_element_type=F32)


def halves(x):
    hi = x.astype(BF16)
    return hi, (x - hi.astype(F32)).astype(BF16)


def mm(a, b, ca=1, cb=0):
    return dg(a[0], b[0], ca, cb) + dg(a[0], b[1], ca, cb) + dg(a[1], b[0], ca, cb)


def thirds(x):
    hi = x.astype(BF16)
    rest = x - hi.astype(F32)
    mid = rest.astype(BF16)
    return hi, mid, (rest - mid.astype(F32)).astype(BF16)


def iota(shape, dim):
    return lax.broadcasted_iota(jnp.int32, shape, dim)


def first_head(rows):
    return iota((rows, LANES), 1) < HEAD


def stacked(x):
    own = first_head(x.shape[0])
    zero = jnp.zeros_like(x)
    return jnp.concatenate([jnp.where(own, x, zero), jnp.where(own, zero, x)], axis=0)


def folded(x):
    half = x.shape[0] // 2
    return x[:half] + x[half:]


def head_ones():
    return (iota((LANES, LANES), 0) // HEAD == iota((LANES, LANES), 1) // HEAD).astype(BF16)


def head_sum(x, ones):
    hi, lo = halves(x)
    return dg(hi, ones) + dg(lo, ones)


def sigmoid(x):
    return 1.0 / (1.0 + jnp.exp(-x))


def mixer_group(first, serve, q_ref, k_ref, v_ref, dip_ref, cri_ref, dco_ref, cro_ref, extra_ref, m_ref, n_ref, r_ref, o_ref):
    ids = range(first, first + GROUP)
    ones = head_ones()
    row, col = iota((LANES, LANES), 0), iota((LANES, LANES), 1)
    eye = (row == col).astype(F32)
    low = (iota((CH, CH), 0) >= iota((CH, CH), 1)).astype(BF16)
    ends, us, bts, avs, reads, vs = [], [], [], [], [], []
    invs, offs, qks = [], [], []
    for c in ids:
        rows = pl.ds(c * CH, CH)
        q, k, v = (r[rows, :].astype(F32) for r in (q_ref, k_ref, v_ref))
        pre = dco_ref[...] + dip_ref[rows, :].astype(F32)
        log_decay = -(sigmoid(pre) * 0.6065306597126334) - extra_ref[rows, :]
        unit = k * lax.rsqrt(head_sum(k * k, ones) + 1e-6)
        b = unit * sigmoid(cro_ref[...] + cri_ref[rows, :].astype(F32))
        total = sum(dg(low, part) for part in thirds(log_decay))
        before = total - log_decay
        mid, end = total[CH // 2 - 1 : CH // 2], total[CH - 1 :]
        up, down = jnp.exp(total - mid), jnp.exp(mid - total)
        up_before = jnp.exp(before - mid)
        rest = jnp.exp(end - total)
        left = halves(jnp.concatenate([stacked(unit * up_before), stacked(q * up)], axis=0))
        right = halves(jnp.concatenate([stacked(k * down), stacked(b * down)], axis=0))
        a = mm(left, right, 1, 1)
        a_uk = jnp.where(row > col, a[:LANES, :LANES], 0.0)
        a_qk = jnp.where(row >= col, a[LANES:, :LANES], 0.0)
        a_qb = jnp.where(row >= col, a[LANES:, LANES:], 0.0)
        offs.append(a[:LANES, LANES:])
        vst = halves(stacked(v))
        av = mm(halves(jnp.concatenate([a_uk, a_qk], axis=0)), vst)
        us.append(halves(jnp.concatenate([stacked(unit * jnp.exp(before)), av[:LANES]], axis=1)))
        avs.append(av[LANES:])
        qks.append(halves(a_qb))
        reads.append(stacked(q * jnp.exp(total)))
        bts.append(halves(stacked(b * rest)))
        ends.append((jnp.exp(end), mm(vst, halves(stacked(k * rest)), 0, 0)))
    serve(first)
    size = 1
    while size < CH:
        inside = (row // (2 * size) == col // (2 * size)) & (row // size != col // size) & (row > col)
        for i in range(GROUP):
            part = jnp.where(inside, offs[i], 0.0)
            if size == 1:
                invs.append(eye - part)
            else:
                inv = halves(invs[i])
                invs[i] = invs[i] - mm(halves(mm(inv, halves(part))), inv)
        size *= 2
    serve(first + 1)
    for i, c in enumerate(ids):
        wu = mm(halves(invs[i]), us[i])
        wu2 = halves(wu)
        ro = mm(qks[i], wu2)
        r_ref[c] = reads[i] - ro[:, :LANES]
        o_ref[c] = avs[i] - ro[:, LANES:]
        mn = mm(wu2, bts[i], 0, 0)
        decay, kv = ends[i]
        m_ref[c] = jnp.where(row == col, decay, 0.0) - mn[:LANES]
        n_ref[c] = kv - mn[LANES:]


def unpacked(message):
    wide = message.astype(F32)
    return stacked(wide[:HEAD]).astype(BF16), stacked(wide[HEAD:])


def packed(trans, state):
    return jnp.concatenate([folded(trans), folded(state)], axis=0).astype(BF16)


def after(total, message):
    trans, state = unpacked(message)
    hi, lo = halves(total)
    out = dg(hi, trans) + dg(lo, trans)
    return jnp.concatenate([out[:LANES], out[LANES:] + state], axis=0)


GQ, GP, DQ, DP = 0, 1, 2, 3
PARTS = ((0, 24, 40, True), (0, 0, 24, False), (1, 16, 16, True), (1, 0, 16, False))
Z_RINGS = (0, 2, 1, 6)
X_RINGS = (0, 16, 8, 17)
DZ = (0, -1, 1, -2, 2, -3, 3, 4)
DX = (0, 1, -1, 2)
Z_ON, Z_FIRST, X_FIRST, X_ON = 0, 1, 2, 3
SCHEDULE = {
    "start": (
        (2, 0, 0, 0), (2, 1, 0, 0), (1, 1, 0, 0), (1, 0, 0, 0),
    ),
    "a0": (
        (2, 3, 0, 0), (1, 3, 0, 0),
    ),
    "a1": (
        (2, 2, 0, 0), (1, 2, 0, 0),
    ),
    "a2": (
        (0, 1, 0, 1),
    ),
    "a3": (
        (2, 0, 1, 0), (3, 1, 0, 0), (0, 0, 0, 1), (1, 1, 1, 0), (1, 1, 2, 0),
    ),
    "a4": (
        (3, 3, 0, 0),
    ),
    "xsent": (
        (2, 0, 2, 0), (3, 0, 0, 0), (0, 1, 0, 2), (3, 0, 1, 0), (2, 0, 3, 0), (2, 0, 4, 0),
        (0, 0, 0, 2),
    ),
    "zsent": (
        (0, 1, 1, 1), (0, 1, 2, 1), (1, 1, 3, 0), (0, 1, 0, 3), (3, 0, 2, 0), (2, 0, 5, 0),
        (2, 0, 6, 0), (0, 0, 0, 3),
    ),
    "z2sent": (
        (3, 0, 3, 0), (0, 1, 1, 2), (0, 1, 2, 2), (3, 0, 4, 0), (0, 1, 3, 1), (2, 0, 7, 0),
        (0, 2, 0, 1), (3, 0, 5, 0), (1, 3, 1, 0),
    ),
    "ag1": (
        (0, 1, 1, 3), (3, 0, 6, 0), (1, 3, 2, 0), (0, 1, 2, 3), (0, 1, 3, 2),
    ),
    "ag2": (
        (3, 2, 0, 0), (1, 3, 3, 0), (2, 2, 1, 0), (0, 2, 0, 2), (2, 2, 2, 0), (3, 0, 7, 0),
        (0, 3, 0, 1),
    ),
    "ag3": (
        (0, 3, 1, 1), (2, 2, 3, 0),
    ),
    "pr0": (
        (0, 1, 3, 3),
    ),
    "pr1": (
        (2, 2, 4, 0), (0, 3, 2, 1),
    ),
    "pr2": (
        (3, 2, 1, 0), (0, 3, 3, 1),
    ),
    "pr3": (
        (3, 2, 2, 0), (2, 2, 5, 0), (0, 2, 0, 3),
    ),
    "gu": (
        (0, 3, 0, 2), (2, 2, 6, 0), (0, 3, 1, 2), (3, 2, 3, 0),
    ),
    "d0": (
        (3, 2, 4, 0), (2, 2, 7, 0), (0, 3, 2, 2), (0, 3, 3, 2),
    ),
    "d1": (
        (3, 2, 5, 0), (0, 3, 0, 3), (3, 2, 6, 0), (0, 3, 1, 3),
    ),
    "d2": (
        (0, 3, 2, 3), (3, 2, 7, 0), (0, 3, 3, 3),
    ),
}


class Gather:
    def __init__(self, bufs, send_z, recv_z, send_x, recv_x, sends):
        self.bufs, self.sends, self.here, self.done = bufs, sends, set(), set()
        self.sems = {"z": (send_z, recv_z), "x": (send_x, recv_x)}
        self.place = {"z": lax.axis_index("z"), "x": lax.axis_index("x")}

    def copy(self, axis, part, i, hop, right, got):
        buf, first, rows, z_first = PARTS[part]
        sign, far = (1 if right else -1), {"z": 4, "x": 2}[axis]
        size = {"z": NZ, "x": NX}
        back = -sign * (hop if got else hop - 1)
        dz, dx = (back, DX[i]) if axis == "z" else (DZ[i], back)
        ref = self.bufs[buf].at[lax.rem(self.place["z"] + dz + NZ, NZ), lax.rem(self.place["x"] + dx + NX, NX)]
        if hop == far:
            cut = (rows // 8 + i % 2) // 2 * 8
            first, rows = (first, cut) if right else (first + cut, rows - cut)
        ref = ref.at[pl.ds(first, rows)]
        ring = (Z_RINGS if axis == "z" else X_RINGS)[part] + i
        slot = hop - 1 + (0 if right else far)
        send, recv = self.sems[axis]
        return pltpu.make_async_remote_copy(
            ref, ref, send.at[ring, slot], recv.at[ring, slot],
            device_id={axis: lax.rem(self.place[axis] + sign + size[axis], size[axis])}, device_id_type=MESH,
        )

    def send(self, axis, part, i, hop):
        for right in (True, False):
            copy = self.copy(axis, part, i, hop, right, False)
            copy.start()
            self.sends.append(copy)

    def need(self, axis, part, i, hop):
        if (axis, part, i, hop) not in self.here:
            self.here.add((axis, part, i, hop))
            for right in (True, False):
                self.copy(axis, part, i, hop, right, True).wait_recv()

    def do(self, kind, part, i, hop):
        self.done.add((kind, part, i, hop))
        z_first = PARTS[part][3]
        if kind == Z_ON:
            self.need("z", part, i, hop)
            self.send("z", part, i, hop + 1)
        elif kind == Z_FIRST:
            if not z_first and i:
                self.need("x", part, 0, 1 if i < 3 else 2)
            self.send("z", part, i, 1)
        elif kind == X_FIRST:
            if z_first and i:
                self.need("z", part, 0, (i + 1) // 2)
            self.send("x", part, i, 1)
        else:
            self.need("x", part, i, 1)
            self.send("x", part, i, 2)

    def serve(self, point):
        for task in SCHEDULE.get(point, ()):
            self.do(*task)

    def whole(self, part):
        for i in range(8 if PARTS[part][3] else 1):
            self.need("x", part, i, 1)
            self.need("x", part, i, 2)
        for i in range(1 if PARTS[part][3] else 4):
            for hop in range(1, 5):
                self.need("z", part, i, hop)

    def slab(self, q, p, i):
        hop = (i + 1) // 2
        if i:
            self.need("z", q, 0, hop)
            for j in range(4):
                self.need("z", p, j, hop)
        for part, ring in ((q, i), (p, 0)):
            self.need("x", part, ring, 1)
            self.need("x", part, ring, 2)


class Spread:
    def __init__(self, block, send_sem, recv_sem, sends):
        self.block, self.send_sem, self.recv_sem, self.sends = block, send_sem, recv_sem, sends
        self.y, self.c = lax.axis_index("y"), lax.axis_index("c")

    def along_y(self, sem, dy, up, half):
        ref = self.block(lax.rem(self.y + dy + NY, NY) * NC + self.c, half)
        return pltpu.make_async_remote_copy(
            ref, ref, self.send_sem.at[sem], self.recv_sem.at[sem],
            device_id={"y": lax.rem(self.y + (1 if up else NY - 1), NY)}, device_id_type=MESH,
        )

    def across(self, sem, dy, mine):
        ref = self.block(lax.rem(self.y + dy + NY, NY) * NC + (self.c if mine else 1 - self.c), None)
        return pltpu.make_async_remote_copy(
            ref, ref, self.send_sem.at[sem], self.recv_sem.at[sem], device_id={"c": 1 - self.c}, device_id_type=MESH
        )

    def go(self, copy):
        copy.start()
        self.sends.append(copy)

    def start(self):
        for half in (0, 1):
            self.go(self.along_y(half, 0, True, half))
            self.go(self.along_y(2 + half, 0, False, 1 - half))
        self.go(self.across(6, 0, True))

    def relay(self):
        self.along_y(0, -1, True, 0).wait_recv()
        self.go(self.along_y(4, -1, True, 0))
        self.along_y(2, 1, False, 1).wait_recv()
        self.go(self.along_y(5, 1, False, 1))

    def near(self):
        self.along_y(1, -1, True, 1).wait_recv()
        self.go(self.across(7, -1, True))
        self.along_y(3, 1, False, 0).wait_recv()
        self.go(self.across(8, 1, True))

    def far(self):
        self.along_y(4, 2, True, 0).wait_recv()
        self.along_y(5, 2, False, 1).wait_recv()
        self.go(self.across(9, 2, True))

    def finish(self):
        for sem, dy in ((6, 0), (7, -1), (8, 1), (9, 2)):
            self.across(sem, dy, False).wait_recv()


_open = []


def mark(name):
    if _open:
        _open.pop().__exit__(None, None, None)
    if name:
        _open.append(jax.named_scope(name))
        _open[-1].__enter__()


def kernel(
    q_hbm, k_hbm, v_hbm, dip_hbm, cri_hbm, dco_hbm, cro_hbm, gain_hbm, extra_t_hbm, fng_hbm,
    resid_hbm, wo_hbm, gate_hbm, up_hbm, down_hbm,
    out_ref,
    q_ref, k_ref, v_ref, dip_ref, cri_ref, dco_ref, cro_ref, gain_ref, extra_t_ref, fng_ref,
    wgu, wd, g_in, u_in, d_in, wo, resid,
    extra_ref, m_ref, n_ref, r_ref, o_ref, gm_ref, hm_ref,
    tot_ref, xbuf, xpre, zsrc, zbuf, s_ref, z2src, z2buf,
    mix_all, mid_ref, rows, hid_ref,
    full_part, own_part, pair, sib_src, sib_buf, far_src, far_buf, y_src, y_buf, far_out, far_in,
    local_sem, send_z, recv_z, send_x, recv_x,
    st_send, st_recv, res_send, res_recv, ag_send, ag_recv, rs_send, rs_recv,
):
    z, x, y, c = (lax.axis_index(n) for n in SP_TP)
    tp = y * NC + c
    sends = []
    tokens, width = rows.shape
    share = tokens // NT

    def block_rows(i):
        return pl.ds(pl.multiple_of(i * share, 16), share)

    def go(copy):
        copy.start()
        sends.append(copy)

    mark("barrier")
    own = [
        pltpu.make_async_copy(src, dst, local_sem.at[i])
        for i, (src, dst) in enumerate(
            ((gate_hbm, g_in), (up_hbm, u_in), (down_hbm, d_in), (resid_hbm, resid.at[block_rows(tp)]),
             (extra_t_hbm, extra_t_ref), (k_hbm, k_ref), (q_hbm, q_ref), (v_hbm, v_ref), (dip_hbm, dip_ref),
             (cri_hbm, cri_ref), (dco_hbm, dco_ref), (cro_hbm, cro_ref), (gain_hbm, gain_ref), (fng_hbm, fng_ref), (wo_hbm, wo))
        )
    ]
    barrier = pltpu.get_barrier_semaphore()
    peers = [{"x": lax.rem(x + d, NX)} for d in range(1, NX)]
    peers += [{"z": lax.rem(z + d, NZ)} for d in range(1, NZ)]
    peers += [{"y": lax.rem(y + d, NY)} for d in range(1, NY)] + [{"c": 1 - c}]
    for copy in own[:3]:
        copy.start()
    for peer in peers:
        pl.semaphore_signal(barrier, inc=1, device_id=peer, device_id_type=MESH)
    for copy in own[3:]:
        copy.start()
    for copy in own[:2]:
        copy.wait()
    hidden = g_in.shape[1]
    full = hidden // LANES * LANES

    def side_by_side(left, right):
        tail = jnp.concatenate([left[:, full:].astype(F32), right[:, full:].astype(F32)], axis=1)
        return jnp.concatenate([left[:, :full], right[:, :full], tail.astype(BF16)], axis=1)

    wgu[z, x] = side_by_side(g_in[...], u_in[...])
    own[2].wait()
    wd[z, x] = side_by_side(d_in[: d_in.shape[0] // 2], d_in[d_in.shape[0] // 2 :])
    own[4].wait()
    extra_t = jnp.concatenate([extra_t_ref[...], jnp.zeros((6, extra_t_ref.shape[1]), F32)], axis=0)
    pick = (iota((8, LANES), 0) == iota((8, LANES), 1) // HEAD).astype(BF16)
    extra_ref[...] = sum(dg(part, pick, 0, 0) for part in thirds(extra_t))
    pl.semaphore_wait(barrier, len(peers))

    g = Gather((wgu, wd), send_z, recv_z, send_x, recv_x, sends)
    g.serve("start")

    def resid_block(i, half):
        cols = pl.ds(0, width) if half is None else pl.ds(half * (width // 2), width // 2)
        return resid.at[block_rows(i), cols]

    def mix_block(i, half):
        part = pl.ds(0, tokens) if half is None else pl.ds(half * (tokens // 2), tokens // 2)
        return mix_all.at[part, pl.ds(pl.multiple_of(i * LANES, LANES), LANES)]

    own[3].wait()
    res = Spread(resid_block, res_send, res_recv, sends)
    res.start()

    mix = functools.partial(
        mixer_group, serve=lambda i: g.serve(f"a{i}"), q_ref=q_ref, k_ref=k_ref, v_ref=v_ref, dip_ref=dip_ref, cri_ref=cri_ref, dco_ref=dco_ref,
        cro_ref=cro_ref, extra_ref=extra_ref, m_ref=m_ref, n_ref=n_ref, r_ref=r_ref, o_ref=o_ref,
    )
    for copy in own[5:14]:
        copy.wait()
    mark("mix0")
    mix(0)
    mark("s1")
    g.serve("a2")
    res.relay()
    mark("mix1")
    mix(GROUP)
    mark("s2")
    g.serve("a5")
    res.near()
    res.far()
    mark("prefix")

    row, col = iota((LANES, LANES), 0), iota((LANES, LANES), 1)
    start = jnp.concatenate([(row == col).astype(F32), jnp.zeros((LANES, LANES), F32)], axis=0)
    total = start
    for i in range(CHUNKS):
        split = halves(total)
        step = mm(split, halves(m_ref[i]))
        gh = mm(halves(r_ref[i]), split, 1, 1)
        rows_i = pl.ds(i * CH, CH)
        gm_ref[rows_i, :] = folded(gh[:, :LANES])
        hm_ref[rows_i, :] = folded(gh[:, LANES:] + o_ref[i])
        total = jnp.concatenate([step[:LANES], step[LANES:] + n_ref[i]], axis=0)
    tot_ref[...] = packed(total[:LANES], total[LANES:])

    def x_state(d):
        return pltpu.make_async_remote_copy(
            tot_ref, xbuf.at[d - 1], st_send.at[d - 1], st_recv.at[d - 1],
            device_id={"x": lax.rem(x + d, NX)}, device_id_type=MESH,
        )

    for d in range(1, NX):
        go(x_state(d))
    mark("s2")
    g.serve("xsent")
    mark("xstate")
    for d in range(1, NX):
        x_state(d).wait_recv()
    mark("xcomb")
    total = start
    prefix = total
    for i in range(NX):
        prefix = jnp.where(x == i, total, prefix)
        message = tot_ref[...]
        for d in range(1, NX):
            message = jnp.where(lax.rem(x - i + NX, NX) == d, xbuf[d - 1], message)
        total = after(total, message)
    xpre[...] = prefix
    zsrc[...] = packed(total[:LANES], total[LANES:])

    place_z, far_half = lax.rem(z, ZG), z >= ZG

    def z_state(d):
        return pltpu.make_async_remote_copy(
            zsrc, zbuf.at[d - 1], st_send.at[NX - 2 + d], st_recv.at[NX - 2 + d],
            device_id={"z": lax.rem(z + d, NZ)}, device_id_type=MESH,
        )

    def z_half(d):
        return pltpu.make_async_remote_copy(
            z2src, z2buf, st_send.at[NX + ZG - 3 + d], st_recv.at[NX + ZG - 2],
            device_id={"z": lax.rem(z + d, NZ)}, device_id_type=MESH,
        )

    for d in range(1, ZG):
        pl.when(place_z + d < ZG)(lambda d=d: z_state(d).start())
    mark("s3")
    g.serve("zsent")
    mark("zstate")
    s_ref[...] = start
    for d in range(ZG - 1, 0, -1):

        @pl.when(place_z >= d)
        def _(d=d):
            z_state(d).wait_recv()
            s_ref[...] = after(s_ref[...], zbuf[d - 1])

    @pl.when(z == ZG - 1)
    def _():
        z2src[...] = folded(after(s_ref[...], zsrc[...])[LANES:]).astype(BF16)
        for d in range(1, ZG + 1):
            z_half(d).start()

    mark("s3b")
    g.serve("z2sent")
    mark("zhalf")

    @pl.when(far_half)
    def _():
        z_half(1).wait_recv()
        s_ref[LANES:] += mm(halves(stacked(z2buf[...].astype(F32))), halves(s_ref[:LANES]))

    mark("read")
    incoming = mm(halves(s_ref[LANES:]), halves(xpre[:LANES])) + xpre[LANES:]
    read = mm(halves(gm_ref[...]), halves(incoming), 1, 1) + hm_ref[...]
    ones = head_ones()
    center = read - head_sum(read, ones) * (1.0 / HEAD)
    spread = head_sum(center * center, ones) * (1.0 / HEAD)
    mine = pl.ds(pl.multiple_of(tp * LANES, LANES), LANES)
    mix_all[:, mine] = (center * lax.rsqrt(spread + 1e-5) * gain_ref[...]).astype(BF16)
    mixed = Spread(mix_block, ag_send, ag_recv, sends)
    mixed.start()
    mark("ag1")
    g.serve("ag1")
    mark("ag1w")
    mixed.relay()
    mark("ag2")
    g.serve("ag2")
    mark("ag2w")
    mixed.near()
    mixed.far()
    mark("ag3")
    g.serve("ag3")
    mark("ag3w")
    own[14].wait()
    res.finish()
    mixed.finish()

    tile = 512
    square = jnp.zeros((tokens, 1), F32)
    for i in range(width // tile):
        mark(f"pr{i}")
        cols = pl.ds(i * tile, tile)
        proj = jnp.dot(mix_all[...], wo[:, cols], preferred_element_type=F32)
        mid = (resid[:, cols].astype(F32) + proj).astype(BF16)
        mid_ref[:, cols] = mid
        mid = mid.astype(F32)
        square += jnp.sum(mid * mid, axis=-1, keepdims=True)
        mark(f"sp{i}")
        g.serve(f"pr{i}")
    mark("norm")
    scale = lax.rsqrt(square * (1.0 / width) + 1e-6)
    for i in range(width // tile):
        cols = pl.ds(i * tile, tile)
        rows[:, cols] = (mid_ref[:, cols].astype(F32) * scale * fng_ref[:, cols]).astype(BF16)
    early = len(sends)
    mark("gu")
    g.serve("gu")
    g.whole(GQ)
    g.whole(GP)

    mark("gateup")
    both = jnp.dot(rows[...], wgu[...].reshape(width, 2 * hidden), preferred_element_type=F32)

    def gated(gate, upper):
        return (gate * sigmoid(gate) * upper).astype(BF16)

    rest = hidden - full
    hid_ref[:, :full] = gated(both[:, :full], both[:, full : 2 * full])
    tail = gated(both[:, 2 * full : 2 * full + rest], both[:, 2 * full + rest :]).astype(F32)
    none = jnp.zeros((tokens, LANES - rest), F32)
    hid_ref[:, full : full + LANES] = jnp.concatenate([tail, none], axis=1).astype(BF16)
    hid_ref[:, full + LANES :] = jnp.concatenate([none, tail], axis=1).astype(BF16)

    slab = width // NZ

    def wide(n):
        return len(COLS[n]) * slab

    def to_mate(n):
        cols = pl.ds(0, wide(n))
        return pltpu.make_async_remote_copy(
            sib_src.at[n, :, :, cols], sib_buf.at[n, :, :, cols], rs_send.at[n, 0], rs_recv.at[n, 0],
            device_id={"c": 1 - c}, device_id_type=MESH,
        )

    def to_y(n, kind, up):
        src, dst = (far_src, far_buf) if kind == 0 else (y_src, y_buf)
        cols = pl.ds(0, wide(n) // 2 if kind == 0 else wide(n))
        k = 0 if up else 1
        sem = 1 + 2 * kind + k
        return pltpu.make_async_remote_copy(
            src.at[n, k, :, cols], dst.at[n, k, :, cols], rs_send.at[n, sem], rs_recv.at[n, sem],
            device_id={"y": lax.rem(y + (1 if up else NY - 1), NY)}, device_id_type=MESH,
        )

    def straight():
        return pltpu.make_async_remote_copy(
            far_out, far_in, rs_send.at[last, 1], rs_recv.at[last, 1],
            device_id={"y": lax.rem(y + 2, NY)}, device_id_type=MESH,
        )

    def place(i):
        return lax.rem(z + DZ[i] + NZ, NZ)

    def product(n):
        for k, i in enumerate(COLS[n]):
            weights = wd[place(i)].reshape(slab // 2, 2 * hidden)
            for side in range(2):
                left = jnp.concatenate([hid_ref[:, :full], hid_ref[:, full + side * LANES : full + (side + 1) * LANES]], axis=1)
                right = jnp.concatenate([weights[:, side * full : (side + 1) * full], weights[:, 2 * full :]], axis=1)
                at = k * slab + side * (slab // 2)
                full_part[n, :, at : at + slab // 2] = dg(left, right, 1, 1)
        for yy in range(NY):
            sib_src[n, yy, :, : wide(n)] = full_part[n, block_rows(yy * NC + 1 - c), : wide(n)].astype(BF16)
        go(to_mate(n))

    def chip_sum(n):
        to_mate(n).wait_recv()
        w, h = wide(n), wide(n) // 2

        def of(d):
            yy = lax.rem(y + d, NY)
            return full_part[n, block_rows(yy * NC + c), :w] + sib_buf[n, yy, :, :w].astype(F32)

        if n == last:
            far_out[...] = of(2).astype(BF16)
            go(straight())
            y_src[n, 0, :, :w] = of(1).astype(BF16)
            go(to_y(n, 1, True))
            y_src[n, 1, :, :w] = of(3).astype(BF16)
            go(to_y(n, 1, False))
            own_part[n, :, :w] = of(0)
            return
        far = of(2).astype(BF16)
        far_src[n, 0, :, :h] = far[:, :h]
        far_src[n, 1, :, :h] = far[:, h:]
        go(to_y(n, 0, True))
        go(to_y(n, 0, False))
        own_part[n, :, :w] = of(0)
        pair[n, 0, :, :w] = of(1)
        pair[n, 1, :, :w] = of(3)

    def ring_sum(n):
        w, h = wide(n), wide(n) // 2
        to_y(n, 0, True).wait_recv()
        y_src[n, 0, :, :h] = (pair[n, 0, :, :h] + far_buf[n, 0, :, :h].astype(F32)).astype(BF16)
        y_src[n, 0, :, h:w] = pair[n, 0, :, h:w].astype(BF16)
        go(to_y(n, 1, True))
        to_y(n, 0, False).wait_recv()
        y_src[n, 1, :, :h] = pair[n, 1, :, :h].astype(BF16)
        y_src[n, 1, :, h:w] = (pair[n, 1, :, h:w] + far_buf[n, 1, :, :h].astype(F32)).astype(BF16)
        go(to_y(n, 1, False))

    def in_order(packed_cols):
        block = slab // NX // 2
        group = iota((share, LANES), 1) // block
        tiles = []
        for t in range(slab // LANES):
            out = None
            for to in range(LANES // block):
                at = LANES // block // 2 * t + to // 2
                shifted = packed_cols[:, (to % 2) * (slab // 2) : (to % 2 + 1) * (slab // 2)]
                shift = (to - at) * block % LANES
                shifted = pltpu.roll(shifted, shift, 1) if shift else shifted
                out = shifted if out is None else jnp.where(group == to, shifted, out)
            tiles.append(out)
        return jnp.concatenate(tiles, axis=1)

    last = len(COLS) - 1

    def finish(n):
        for up in (True, False):
            to_y(n, 1, up).wait_recv()
        if n == last:
            straight().wait_recv()
        for k, i in enumerate(COLS[n]):
            at = slice(k * slab, (k + 1) * slab)
            acc = own_part[n, :, at] + y_buf[n, 0, :, at].astype(F32) + y_buf[n, 1, :, at].astype(F32)
            if n == last:
                acc += far_in[...].astype(F32)
            acc = in_order(acc)
            cols = pl.ds(pl.multiple_of(place(i) * slab, slab), slab)
            out_ref[:, cols] = (mid_ref[block_rows(tp), cols].astype(F32) + 0.5 * acc).astype(BF16)

    for n in range(len(COLS)):
        mark(f"d{n}")
        g.serve(f"d{n}")
        if n > 0:
            chip_sum(n - 1)
        if n > 1:
            ring_sum(n - 2)
        if n == last:
            for copy in sends[:early]:
                copy.wait_send()
        mark(f"w{n}")
        for i in COLS[n]:
            g.slab(DQ, DP, i)
        mark(f"p{n}")
        product(n)
    mark("rs2")
    ring_sum(last - 1)
    mark("cs3")
    chip_sum(last)
    mark("fin0")
    for n in range(last - 1):
        finish(n)
    mark("fin2")
    finish(last - 1)
    mark("fin3")
    finish(last)
    mark("sendwait")
    for copy in sends[early:]:
        copy.wait_send()
    for d in range(1, ZG):
        pl.when(place_z + d < ZG)(lambda d=d: z_state(d).wait_send())

    @pl.when(z == ZG - 1)
    def _():
        for d in range(1, ZG + 1):
            z_half(d).wait_send()

    mark(None)


def per_device(
    resid, queries, keys, values, decay_input_part, decay_channel_offset, decay_head_extra, correction_rate_input,
    correction_rate_offset, head_norm_gain, mixer_output_weight, feedforward_norm_gain, gate_weight, up_weight, down_weight,
):
    tokens = queries.shape[0]
    share, width = resid.shape
    shard, hidden = gate_weight.shape
    vm, sem = pltpu.VMEM, pltpu.SemaphoreType.DMA
    flat = pl.BlockSpec(memory_space=pltpu.VMEM)
    there = pl.BlockSpec(memory_space=pl.ANY)
    slab = width // NZ
    parts, wide = len(COLS), max(map(len, COLS)) * slab
    return pl.pallas_call(
        kernel,
        name="layer",
        out_shape=pltpu.VMEM((share, width), BF16),
        in_specs=[there] * 15,
        out_specs=flat,
        scratch_shapes=[
            *[vm((tokens, LANES), BF16)] * 5, *[vm((1, LANES), F32)] * 3, vm((LANES // HEAD, tokens), F32), vm((1, width), F32),
            vm((NZ, NX, shard, 2 * hidden), BF16), vm((NZ, NX, shard // 2, 2 * hidden), BF16),
            vm((shard, hidden), BF16), vm((shard, hidden), BF16), vm((shard, hidden), BF16),
            vm(mixer_output_weight.shape, BF16), vm((tokens, width), BF16),
            vm((tokens, LANES), F32),
            vm((CHUNKS, LANES, LANES), F32), vm((CHUNKS, LANES, LANES), F32),
            vm((CHUNKS, LANES, LANES), F32), vm((CHUNKS, LANES, LANES), F32),
            vm((tokens, LANES), F32), vm((tokens, LANES), F32),
            vm((LANES, LANES), BF16), vm((NX - 1, LANES, LANES), BF16), vm((2 * LANES, LANES), F32),
            vm((LANES, LANES), BF16), vm((ZG - 1, LANES, LANES), BF16), vm((2 * LANES, LANES), F32),
            vm((HEAD, LANES), BF16), vm((HEAD, LANES), BF16),
            vm((tokens, NT * LANES), BF16), vm((tokens, width), BF16), vm((tokens, width), BF16), vm((tokens, hidden // LANES * LANES + 2 * LANES), BF16),
            vm((parts, tokens, wide), F32), vm((parts, share, wide), F32), vm((parts, 2, share, wide), F32),
            vm((parts, NY, share, wide), BF16), vm((parts, NY, share, wide), BF16),
            vm((parts, 2, share, wide // 2), BF16), vm((parts, 2, share, wide // 2), BF16),
            vm((parts, 2, share, wide), BF16), vm((parts, 2, share, wide), BF16),
            vm((share, len(COLS[-1]) * slab), BF16), vm((share, len(COLS[-1]) * slab), BF16),
            sem((15,)), sem((10, 8)), sem((10, 8)), sem((18, 4)), sem((18, 4)),
            sem((NX + 2 * ZG - 2,)), sem((NX + ZG - 1,)), sem((10,)), sem((10,)), sem((10,)), sem((10,)),
            sem((parts, 5)), sem((parts, 5)),
        ],
        compiler_params=pltpu.CompilerParams(collective_id=0, has_side_effects=True),
    )(
        queries, keys, values, decay_input_part, correction_rate_input,
        decay_channel_offset[None], correction_rate_offset[None], head_norm_gain[None], decay_head_extra.T,
        feedforward_norm_gain[None], resid, mixer_output_weight, gate_weight, up_weight, down_weight.T,
    )


def solution(mesh):
    torus = Mesh(mesh.devices.reshape(NZ, NX, NY, NC), SP_TP)
    in_specs = (
        P(SP_TP, None), P(SP, TP), P(SP, TP), P(SP, TP), P(SP, TP), P(TP), P(SP, TP), P(SP, TP), P(TP), P(TP),
        P(), P(), P(SP, TP), P(SP, TP), P(TP, SP),
    )
    return jax.shard_map(per_device, mesh=torus, in_specs=in_specs, out_specs=P(SP_TP, None), check_vma=False)
```
